256 devices in a mesh: sp: 32 (over z, y), tp: 8 (over x, core).
Axes of the slice: x: 4, y: 4, z: 8, core: 2. Of those that a mesh axis runs over, the one named last changes fastest.
Arguments:
- latents: bfloat16 [10240, 2048], P(('sp', 'tp')), may hold values from -12.5 to 12.5, as said below
- context: bfloat16 [1024, 2048], P('sp'), may hold values from -120 to 120, as said below
- cond_vec: float32 [2048], replicated, may hold values from -6 to 6
- ctx_vec: float32 [2048], replicated, may hold values from -6 to 6
- shift_w: bfloat16 [2048, 2048], P('sp', 'tp'), may hold values from -0.125 to 0.125
- scale_w: bfloat16 [2048, 2048], P('sp', 'tp'), may hold values from -0.125 to 0.125
- modgate_w: bfloat16 [2048, 2048], P('sp', 'tp'), may hold values from -0.125 to 0.125
- query_down_weight: bfloat16 [2048, 512], replicated, may hold values from -0.125 to 0.125
- latent_down_weight: bfloat16 [2048, 256], replicated, may hold values from -0.125 to 0.125
- rot_down: bfloat16 [2048, 32], replicated, may hold values from -0.125 to 0.125
- gate_w: bfloat16 [2048, 2048], P(None, 'tp'), may hold values from -0.125 to 0.125
- query_norm_gain: float32 [512], replicated, may hold values from 0.1 to 1.9
- latent_norm_gain: float32 [256], replicated, may hold values from 0.1 to 1.9
- query_plain_weight: bfloat16 [512, 2048], P(None, 'tp'), may hold values from -0.25 to 0.25
- query_rotary_weight: bfloat16 [512, 1024], P(None, 'tp'), may hold values from -0.25 to 0.25
- key_expand_weight: bfloat16 [256, 2048], P(None, 'tp'), may hold values from -0.375 to 0.375
- value_expand_weight: bfloat16 [256, 2048], P(None, 'tp'), may hold values from -0.375 to 0.375
- out_w: bfloat16 [2048, 2048], P('tp'), may hold values from -0.5 to 0.5
- norm_gain: float32 [2048], replicated, may hold values from 0.1 to 1.9
- norm_bias: float32 [2048], replicated, may hold values from -3 to 3
Outputs:
- mixed_out: bfloat16 [10240, 2048], P(('sp', 'tp'))
The draws below stay inside these ranges and needn't reach their ends.
Inputs may be any that keep to these rules, and one draw needn't show every extreme that they name: `latents`: latent rows are noise plus three slow waves along the whole sequence. Most context rows have their own scales of 1 to 3; a few rows may be far larger.
All inputs are finite; a program needn't handle non-finite values.
Results may differ from the reference program's by a relative error of at most 0.024.
The reference program's roundings to bfloat16 on the way count: a program that leaves them out, or rounds other values in their place, can miss the bound.
Values may be sent and summed in bfloat16 or wider, within the bound.
A program may use at most 128 MiB of HBM per device.

```python
import math
import jax
import jax.numpy as jnp
from jax import lax

MODEL_WIDTH = 2048
HEAD_COUNT = 32
QUERY_LATENT = 512
LATENT_WIDTH = 256
PLAIN_HEAD_SIZE = 64
ROTARY_SIZE = 32
VALUE_HEAD_SIZE = 64
GRID_W = 64
TOK_DEV = 320
CTX = 1024
TOKENS = 10240
N_TP = 8


def draw_latents(key, part):
    noise_key, wave_key, phase_key = jax.random.split(key, 3)
    noise_part = jnp.clip(jax.random.normal(noise_key, (TOKENS, MODEL_WIDTH), jnp.float32), -5.0, 5.0)
    directions = jnp.clip(jax.random.normal(wave_key, (3, MODEL_WIDTH), jnp.float32), -2.5, 2.5)
    phases = jax.random.uniform(phase_key, (3,), jnp.float32, 0.0, 2.0 * math.pi)
    position = jnp.arange(TOKENS, dtype=jnp.float32) / TOKENS
    frequency = jnp.arange(1, 4, dtype=jnp.float32)
    wave_part = jnp.cos(2.0 * math.pi * position[:, None] * frequency[None, :] + phases[None, :])
    return (noise_part + wave_part @ directions).astype(jnp.bfloat16)


def draw_context(key, part):
    value_key, scale_key, pick_key, large_key = jax.random.split(key, 4)
    row_scale = jnp.exp(jax.random.uniform(scale_key, (CTX, 1), jnp.float32, 0.0, math.log(3.0)))
    values = jnp.clip(jax.random.normal(value_key, (CTX, MODEL_WIDTH), jnp.float32), -6.0, 6.0) * row_scale
    return values.astype(jnp.bfloat16)


def level_of(own_key, shape, cuts, smallest, largest):
    loudness, own = 1.0, jax.random.fold_in(own_key, 6)
    for dim, blocks in cuts:
        heights = jnp.exp(jax.random.uniform(jax.random.fold_in(own, dim), (blocks,), jnp.float32, smallest / len(cuts), largest / len(cuts)))
        loudness = loudness * jnp.repeat(heights, shape[dim] // blocks).reshape([-1 if axis == dim else 1 for axis in range(len(shape))])
    return loudness


def bell_draw(rng, extent, scale, limit, cuts=(), kind=jnp.bfloat16):
    factor_of = level_of(rng, extent, cuts, -0.22, 0.18) if cuts else 1.0
    drawn = jax.random.normal(rng, extent, jnp.float32) * scale * factor_of
    return jnp.minimum(jnp.maximum(drawn, -limit), limit).astype(kind)


def setup_inputs(seed: int = 0) -> dict:
    keys = jax.random.split(jax.random.key(seed), 21)
    return {
        "latents": draw_latents(jax.random.fold_in(keys[20], 71), 0),
        "context": draw_context(jax.random.fold_in(keys[20], 71), 0),
        "cond_vec": bell_draw(keys[2], (MODEL_WIDTH,), 1.0, 6.0, (), jnp.float32),
        "ctx_vec": bell_draw(keys[3], (MODEL_WIDTH,), 1.0, 6.0, (), jnp.float32),
        "shift_w": bell_draw(keys[4], (MODEL_WIDTH, MODEL_WIDTH), MODEL_WIDTH ** -0.5, 0.125, ((0, 32), (1, 8))),
        "scale_w": bell_draw(keys[5], (MODEL_WIDTH, MODEL_WIDTH), MODEL_WIDTH ** -0.5, 0.125, ((0, 32), (1, 8))),
        "modgate_w": bell_draw(keys[6], (MODEL_WIDTH, MODEL_WIDTH), MODEL_WIDTH ** -0.5, 0.125, ((0, 32), (1, 8))),
        "query_down_weight": bell_draw(keys[7], (MODEL_WIDTH, QUERY_LATENT), MODEL_WIDTH ** -0.5, 0.125),
        "latent_down_weight": bell_draw(keys[8], (MODEL_WIDTH, LATENT_WIDTH), MODEL_WIDTH ** -0.5, 0.125),
        "rot_down": bell_draw(keys[9], (MODEL_WIDTH, ROTARY_SIZE), MODEL_WIDTH ** -0.5, 0.125),
        "gate_w": bell_draw(keys[10], (MODEL_WIDTH, HEAD_COUNT * VALUE_HEAD_SIZE), MODEL_WIDTH ** -0.5, 0.125, ((1, 8),)),
        "query_norm_gain": jnp.clip(1.0 + 0.18 * jax.random.normal(keys[11], (QUERY_LATENT,), jnp.float32), 0.1, 1.9),
        "latent_norm_gain": jnp.clip(1.0 + 0.18 * jax.random.normal(keys[12], (LATENT_WIDTH,), jnp.float32), 0.1, 1.9),
        "query_plain_weight": bell_draw(keys[13], (QUERY_LATENT, HEAD_COUNT * PLAIN_HEAD_SIZE), QUERY_LATENT ** -0.5, 0.25, ((1, 8),)),
        "query_rotary_weight": bell_draw(keys[14], (QUERY_LATENT, HEAD_COUNT * ROTARY_SIZE), QUERY_LATENT ** -0.5, 0.25, ((1, 8),)),
        "key_expand_weight": bell_draw(keys[15], (LATENT_WIDTH, HEAD_COUNT * PLAIN_HEAD_SIZE), LATENT_WIDTH ** -0.5, 0.375, ((1, 8),)),
        "value_expand_weight": bell_draw(keys[16], (LATENT_WIDTH, HEAD_COUNT * VALUE_HEAD_SIZE), LATENT_WIDTH ** -0.5, 0.375, ((1, 8),)),
        "out_w": bell_draw(keys[17], (HEAD_COUNT * VALUE_HEAD_SIZE, MODEL_WIDTH), (HEAD_COUNT * VALUE_HEAD_SIZE // 16) ** -0.5, 0.5, ((0, 8),)),
        "norm_gain": jnp.clip(1.0 + 0.18 * jax.random.normal(keys[18], (MODEL_WIDTH,), jnp.float32), 0.1, 1.9),
        "norm_bias": bell_draw(keys[19], (MODEL_WIDTH,), 0.5, 3.0, (), jnp.float32),
    }


rope_base = 10000.0
norm_floor = 1e-06
residual_weight = 2.0 ** 0.5

def rms_scale(values, gain):
    return values * lax.rsqrt(lax.optimization_barrier(jnp.mean(values * values, axis=-1, keepdims=True)) + norm_floor) * gain

def rotate(values, positions):
    pair_count = ROTARY_SIZE // 4
    inverse = rope_base ** (-jnp.arange(pair_count, dtype=jnp.float32) / pair_count)
    grid_row = (positions // GRID_W).astype(jnp.float32)
    grid_col = (positions % GRID_W).astype(jnp.float32)
    angles = jnp.stack([grid_row[:, None] * inverse, grid_col[:, None] * inverse], axis=1)
    cosine = jnp.cos(angles)[:, None, :, None, :]
    sine_part = jnp.sin(angles)[:, None, :, None, :]
    shaped = values.reshape(values.shape[0], -1, 2, 2, pair_count)
    first_part = shaped[:, :, :, 0:1, :]
    second = shaped[:, :, :, 1:2, :]
    turned = jnp.concatenate([first_part * cosine - second * sine_part, second * cosine + first_part * sine_part], axis=3)
    return turned.reshape(values.shape)

def project(rows, weight):
    return jnp.dot(rows, weight, preferred_element_type=jnp.float32)

def reference(latents, context, cond_vec, ctx_vec, shift_w, scale_w, modgate_w, query_down_weight, latent_down_weight, rot_down, gate_w, query_norm_gain, latent_norm_gain, query_plain_weight, query_rotary_weight, key_expand_weight, value_expand_weight, out_w, norm_gain, norm_bias):
    cond_rows = jnp.stack([jax.nn.silu(cond_vec), jax.nn.silu(ctx_vec)]).astype(jnp.bfloat16)
    shift_vec = project(cond_rows, shift_w)
    scale_vec = project(cond_rows, scale_w)
    gate_vec = project(cond_rows, modgate_w)
    latent_in = (latents.astype(jnp.float32) * (1.0 + scale_vec[0]) + shift_vec[0]).astype(jnp.bfloat16)
    context_in = (context.astype(jnp.float32) * (1.0 + scale_vec[1]) + shift_vec[1]).astype(jnp.bfloat16)
    positions = jnp.arange(TOKENS, dtype=jnp.int32)
    q_codes = rms_scale(project(latent_in, query_down_weight), query_norm_gain).astype(jnp.bfloat16)
    q_cont = project(q_codes, query_plain_weight).astype(jnp.bfloat16).reshape(TOKENS, HEAD_COUNT, PLAIN_HEAD_SIZE)
    q_rot = rotate(project(q_codes, query_rotary_weight), positions).astype(jnp.bfloat16).reshape(TOKENS, HEAD_COUNT, ROTARY_SIZE)
    gate_act = project(latent_in, gate_w).astype(jnp.bfloat16)
    all_in = jnp.concatenate([context_in, latent_in], axis=0)
    kv_codes = rms_scale(project(all_in, latent_down_weight), latent_norm_gain).astype(jnp.bfloat16)
    key_rot = jnp.concatenate([project(context_in, rot_down), rotate(project(latent_in, rot_down), positions)], axis=0).astype(jnp.bfloat16)
    key_rows = project(kv_codes, key_expand_weight).astype(jnp.bfloat16).reshape(-1, HEAD_COUNT, PLAIN_HEAD_SIZE).astype(jnp.float32)
    value_rows = project(kv_codes, value_expand_weight).astype(jnp.bfloat16).reshape(-1, HEAD_COUNT, VALUE_HEAD_SIZE).astype(jnp.float32)
    rot_wide = key_rot.astype(jnp.float32)
    score_scale = (PLAIN_HEAD_SIZE + ROTARY_SIZE) ** (-0.5)
    block_rows = TOK_DEV // N_TP

    def attend_block(inputs):
        cont_block, rot_block = inputs
        scores = jnp.einsum('qhd,khd->hqk', cont_block.astype(jnp.float32), key_rows)
        scores = (scores + jnp.einsum('qhd,kd->hqk', rot_block.astype(jnp.float32), rot_wide)) * score_scale
        weights = jnp.exp(scores - lax.optimization_barrier(jnp.max(scores, axis=-1, keepdims=True)))
        weights_low = lax.optimization_barrier(weights.astype(jnp.bfloat16)).astype(jnp.float32)
        weighted = jnp.einsum('hqk,khd->qhd', weights_low, value_rows)
        return weighted / jnp.transpose(lax.optimization_barrier(jnp.sum(weights, axis=-1)))[:, :, None]
    blocks = TOKENS // block_rows
    attended = lax.map(attend_block, (q_cont.reshape(blocks, block_rows, HEAD_COUNT, PLAIN_HEAD_SIZE), q_rot.reshape(blocks, block_rows, HEAD_COUNT, ROTARY_SIZE)))
    attended = attended.reshape(TOKENS, HEAD_COUNT * VALUE_HEAD_SIZE)
    gated = (attended * jax.nn.silu(gate_act.astype(jnp.float32))).astype(jnp.bfloat16)
    branch = project(gated, out_w)
    blended = residual_weight * latents.astype(jnp.float32) + gate_vec[0] * branch
    row_mean = lax.optimization_barrier(jnp.mean(blended, axis=-1, keepdims=True))
    centred = blended - row_mean
    row_var = lax.optimization_barrier(jnp.mean(centred * centred, axis=-1, keepdims=True))
    return (centred * lax.rsqrt(row_var + norm_floor) * norm_gain + norm_bias).astype(jnp.bfloat16)
```

```python
import math

import jax
import jax.numpy as jnp
import numpy as np
from jax import lax
from jax.experimental import pallas as pl
from jax.experimental.pallas import tpu as pltpu
from jax.sharding import PartitionSpec as P

F32, BF16 = jnp.float32, jnp.bfloat16
NZ, NY, NX, NC = 8, 4, 4, 2
NTP = NX * NC
ROWS = 40
SLAB = 320
HALF = 160
CTXH = 16
PIECE = HALF + CTXH
MSG = PIECE + 32
CUT = 112
UNIT = 2 * NY * PIECE
WIDTH = 2048
COL = 256
EPS = 1e-06
SQRT2 = 2.0**0.5
SCORE = math.log2(math.e) / math.sqrt(96.0)


def rope_tables():
    inverse = (10000.0 ** (-np.arange(8, dtype=np.float64) / 8)).astype(np.float32)
    lane = np.arange(128)
    axis, member, pair = (lane // 16) % 2, (lane // 8) % 2, lane % 8
    sign = np.where(member == 0, -1.0, 1.0)

    def rows_of(numbers, which):
        angle = (numbers[:, None].astype(np.float32) * inverse[pair][None, :]).astype(np.float64)
        keep = axis[None, :] == which
        return np.where(keep, np.cos(angle), 0.0), np.where(keep, np.sin(angle) * sign, 0.0)

    cos_row, sin_row = rows_of(np.arange(160), 0)
    cos_col, sin_col = rows_of(np.arange(64), 1)
    by_slab = np.zeros((32, 16, 128), np.float32)
    by_slab[:, 0:5] = cos_row.reshape(32, 5, 128)
    by_slab[:, 8:13] = sin_row.reshape(32, 5, 128)
    return by_slab, np.concatenate([cos_col, sin_col], 0).astype(np.float32)


def dot(a, b):
    return jnp.dot(a, b, preferred_element_type=F32)


def silu(v):
    return v / (1.0 + jnp.exp(-v))


def rms(v, gain):
    return v * lax.rsqrt(jnp.mean(v * v, axis=-1, keepdims=True) + EPS) * gain


def swap_members(v):
    lane = lax.broadcasted_iota(jnp.int32, v.shape, 1)
    return jnp.where(lane % 16 < 8, pltpu.roll(v, 120, 1), pltpu.roll(v, 8, 1))


def body(
    lat_h, ctx_h, cond_h, ctxv_h, shw_h, scw_h, mgw_h, qd_h, ld_h, rd_h, gw_h, qg_h, kg_h, qp_h, qr_h, ke_h, ve_h,
    ow_h, ng_h, nb_h, rrow_h, rcol_h, out,
    gath, ctx_v, cond_v, ctxv_v, w3, qd, ld, rd, gw, qg, kg, qp, qr, ke, ve, ow, ng, nb, rrow, rcol,
    ybuf, zbuf, mod, xin, xc, tabc, tabs, kv, ket, q2, kt2, acc, top, total, sgate, gsrc, gdst,
    lsem, ysend, yrecv, zsend, zrecv, tsend, trecv, lx_send, lx_recv, kz_send, kz_recv, ky_send, ky_recv,
    kd_send, kd_recv, ox_send, ox_recv, a_send, a_recv,
):
    sp, tp = lax.axis_index("sp"), lax.axis_index("tp")
    z, y, x, c = sp // NY, sp % NY, tp // NC, tp % NC

    def at_z(d):
        return {"sp": ((z + d) % NZ) * NY + y, "tp": tp}

    def at_y(d):
        return {"sp": z * NY + (y + d) % NY, "tp": tp}

    def slot_x(d):
        return ((x + d) % NX) * NC + c

    def at_x(d):
        return {"sp": sp, "tp": slot_x(d)}

    partner_slot = x * NC + (1 - c)
    partner = {"sp": sp, "tp": partner_slot}

    def at_tp(d):
        return {"sp": sp, "tp": (tp + d) % NTP}

    def push(src, dst, send, recv, to):
        pltpu.make_async_remote_copy(
            src_ref=src, dst_ref=dst, send_sem=send, recv_sem=recv, device_id=to, device_id_type=pl.DeviceIdType.MESH
        ).start()

    def take(ref, sem):
        pltpu.make_async_copy(ref, ref, sem).wait()

    local = [
        (cond_h, cond_v), (ctxv_h, ctxv_v), (shw_h, w3.at[0]), (scw_h, w3.at[1]), (mgw_h, w3.at[2]),
        (lat_h, gath.at[tp]), (ctx_h, ctx_v), (ld_h, ld), (rd_h, rd), (rrow_h.at[sp], rrow), (rcol_h, rcol),
        (kg_h, kg), (qd_h, qd), (qg_h, qg), (qp_h, qp), (qr_h, qr), (gw_h, gw), (ke_h, ke), (ve_h, ve),
        (ow_h, ow.at[tp]), (ng_h, ng), (nb_h, nb),
    ]
    for k, (src, dst) in enumerate(local):
        pltpu.make_async_copy(src, dst, lsem.at[k]).start()

    def have(*which):
        for k in which:
            take(local[k][1], lsem.at[k])

    barrier = pltpu.get_barrier_semaphore()
    peers = [at_y(d) for d in range(1, NY)] + [at_z(d) for d in range(1, NZ)] + [at_tp(d) for d in range(1, NTP)]
    for peer in peers:
        pl.semaphore_signal(barrier, inc=1, device_id=peer, device_id_type=pl.DeviceIdType.MESH)

    have(0, 1, 2, 3, 4)
    pick = pl.ds(sp // 2, 1)
    lane = lax.broadcasted_iota(jnp.int32, (8, 128), 1)
    line = lax.broadcasted_iota(jnp.int32, (8, 128), 0)
    mine = lane // 64 == sp % 2
    cond_row = jnp.broadcast_to(silu(cond_v[pick, :]), (8, 128))
    ctxv_row = jnp.broadcast_to(silu(ctxv_v[pick, :]), (8, 128))
    part = jnp.zeros((8, COL), F32)
    for k in range(3):
        rows = jnp.where(line == 2 * k, cond_row, jnp.where(line == 2 * k + 1, ctxv_row, 0.0))
        rows = jnp.where(mine, rows, 0.0).astype(BF16)
        part = part + dot(rows, jnp.concatenate([w3[k], w3[k]], axis=0))
    ybuf[y] = part
    pl.semaphore_wait(barrier, len(peers))

    for d in range(1, NY):
        push(ybuf.at[y], ybuf.at[y], ysend.at[d - 1], yrecv.at[d - 1], at_y(d))
    have(5)
    own = gath.at[tp]
    push(own, own, lx_send.at[0], lx_recv.at[0], at_x(1))
    push(own, own, lx_send.at[1], lx_recv.at[1], at_x(-1))
    push(own, own, lx_send.at[2], lx_recv.at[2], partner)
    for d in range(1, NY):
        take(ybuf.at[(y - d) % NY], yrecv.at[d - 1])
    zbuf[z] = (ybuf[0] + ybuf[1]) + (ybuf[2] + ybuf[3])
    for d in range(1, NZ):
        push(zbuf.at[z], zbuf.at[z], zsend.at[d - 1], zrecv.at[d - 1], at_z(d))

    left, right, across = slot_x(-1), slot_x(1), slot_x(2)
    first, second = pl.ds(0, WIDTH // 2), pl.ds(WIDTH // 2, WIDTH // 2)
    take(gath.at[left], lx_recv.at[0])
    push(gath.at[left, :, first], gath.at[left, :, first], lx_send.at[3], lx_recv.at[3], at_x(1))
    push(gath.at[left], gath.at[left], lx_send.at[4], lx_recv.at[4], partner)
    take(gath.at[right], lx_recv.at[1])
    push(gath.at[right, :, second], gath.at[right, :, second], lx_send.at[5], lx_recv.at[5], at_x(-1))
    push(gath.at[right], gath.at[right], lx_send.at[6], lx_recv.at[6], partner)

    for d in range(1, NZ):
        take(zbuf.at[(z - d) % NZ], zrecv.at[d - 1])
    whole = zbuf[0]
    for k in range(1, NZ):
        whole = whole + zbuf[k]
    mod[tp] = whole
    for d in range(1, NTP):
        push(mod.at[tp], mod.at[tp], tsend.at[d - 1], trecv.at[d - 1], at_tp(d))

    have(9, 10, 17)
    for k in range(5):
        rows = pl.ds(64 * k, 64)
        tabc[rows, :] = rrow[k : k + 1, :] + rcol[0:64, :]
        tabs[rows, :] = rrow[8 + k : 9 + k, :] + rcol[64:128, :]
    ket[...] = ke[...].astype(F32).T.astype(BF16)
    top[...] = jnp.full(top.shape, -1e30, F32)
    total[...] = jnp.zeros(total.shape, F32)
    acc[...] = jnp.zeros(acc.shape, F32)

    take(gath.at[across, :, first], lx_recv.at[3])
    take(gath.at[across, :, second], lx_recv.at[5])
    push(gath.at[across], gath.at[across], lx_send.at[7], lx_recv.at[7], partner)

    for d in range(1, NTP):
        take(mod.at[(tp - d) % NTP], trecv.at[d - 1])
    have(19)
    owned = ow.at[tp]
    push(owned, owned, ox_send.at[0], ox_recv.at[0], at_x(1))
    push(owned, owned, ox_send.at[1], ox_recv.at[1], at_x(-1))
    push(owned, owned, ox_send.at[2], ox_recv.at[2], partner)

    def vector(row):
        return jnp.concatenate([mod[t, row : row + 1, :] for t in range(NTP)], axis=1)

    take(gath.at[partner_slot], lx_recv.at[2])
    for n, d in ((4, -1), (6, 1), (7, 2)):
        take(gath.at[((x + d) % NX) * NC + (1 - c)], lx_recv.at[n])
    shift, scale = vector(0), 1.0 + vector(2)
    for p in range(NTP // 2):
        pair = jnp.concatenate([gath[2 * p].astype(F32), gath[2 * p + 1].astype(F32)], axis=0)
        xin[2 * ROWS * p : 2 * ROWS * (p + 1), :] = (pair * scale + shift).astype(BF16)
    have(6)
    xc[...] = (ctx_v[...].astype(F32) * (1.0 + vector(3)) + vector(1)).astype(BF16)

    have(7, 8, 11)
    half = pl.ds(pl.multiple_of(HALF * c, HALF), HALF)
    mine_in = jnp.concatenate([xin[half, :], xc[pl.ds(pl.multiple_of(CTXH * c, CTXH), CTXH), :]], axis=0)
    slot = NY * c + y
    kv[z, slot, 0:PIECE, :] = rms(dot(mine_in, ld[...]), kg[...]).astype(BF16)
    flat = jnp.concatenate([dot(mine_in, rd[...]), jnp.zeros((PIECE, 96), F32)], axis=1)
    lat_part = flat[0:HALF]
    turned = lat_part * tabc[half, :] + swap_members(lat_part) * tabs[half, :]
    both = jnp.concatenate([turned, flat[HALF:], jnp.zeros((256 - PIECE, 128), F32)], axis=0)
    kv[z, slot, PIECE:MSG, :] = both.T[0:32, :].astype(BF16)

    def z_of(i):
        off = (i % 2) * ((i + 1) // 2) - (1 - i % 2) * (i // 2)
        return (z + off + NZ) % NZ

    low, high = pl.ds(0, CUT), pl.ds(CUT, MSG - CUT)

    def stage_z(i):
        here = kv.at[z_of(i), slot]

        def when(test, act):
            if isinstance(test, bool):
                if test:
                    act()
            else:
                pl.when(test)(act)

        def forward_whole():
            to = {"sp": ((z + NZ + 1 - 2 * (i % 2)) % NZ) * NY + y, "tp": tp}
            push(here, here, kz_send.at[i + 2], kz_recv.at[i + 2], to)

        def forward_low():
            push(here.at[low], here.at[low], kz_send.at[7], kz_recv.at[7], at_z(-1))

        def forward_high():
            push(here.at[high], here.at[high], kz_send.at[8], kz_recv.at[8], at_z(1))

        def take_whole():
            take(here, kz_recv.at[i])

        def take_parts():
            take(here.at[low], kz_recv.at[7])
            take(here.at[high], kz_recv.at[8])

        if isinstance(i, int) and i == 0:
            push(here, here, kz_send.at[1], kz_recv.at[1], at_z(-1))
            push(here, here, kz_send.at[2], kz_recv.at[2], at_z(1))
        else:
            when(i < 7, take_whole)
            when(i == 7, take_parts)
            when(i < 5, forward_whole)
            when(i == 5, forward_low)
            when(i == 6, forward_high)
        push(here, here, ky_send.at[i, 0], ky_recv.at[i, 0], at_y(1))
        push(here, here, ky_send.at[i, 1], ky_recv.at[i, 1], at_y(-1))

    def at_slot(i, d):
        return kv.at[z_of(i), NY * c + (y + d + NY) % NY]

    def stage_y(i):
        below, above = at_slot(i, -1), at_slot(i, 1)
        take(below, ky_recv.at[i, 0])
        push(below.at[low], below.at[low], ky_send.at[i, 2], ky_recv.at[i, 2], at_y(1))
        take(above, ky_recv.at[i, 1])
        push(above.at[high], above.at[high], ky_send.at[i, 3], ky_recv.at[i, 3], at_y(-1))

    def stage_d(i):
        far = at_slot(i, 2)
        take(far.at[low], ky_recv.at[i, 2])
        take(far.at[high], ky_recv.at[i, 3])
        four = kv.at[z_of(i), pl.ds(NY * c, NY)]
        push(four, four, kd_send.at[i], kd_recv.at[i], partner)

    stage_z(0)

    have(12, 13, 14, 15)
    q_codes = rms(dot(xin[...], qd[...]), qg[...]).astype(BF16)
    q_cont = dot(q_codes, qp[...]) * SCORE
    q_rot = dot(q_codes, qr[...])
    q_rot = (q_rot * tabc[...] + swap_members(q_rot) * tabs[...]) * SCORE
    q_lane = lax.broadcasted_iota(jnp.int32, (SLAB, 128), 1)
    for h in range(4):
        j, rows = h // 2, pl.ds(SLAB * (h % 2), SLAB)
        plain = q_cont[:, 128 * j : 128 * (j + 1)]
        q2[j, rows, 0:128] = jnp.where(q_lane // 64 == h % 2, plain, 0.0).astype(BF16)
        q2[j, rows, 128:256] = jnp.where(q_lane // 32 == h, q_rot, 0.0).astype(BF16)
    stage_z(1)
    stage_y(0)
    have(16)
    sgate[...] = silu(dot(xin[...], gw[...]).astype(BF16).astype(F32))
    stage_z(2)
    stage_y(1)
    stage_d(0)

    def one_unit(i, carry):
        @pl.when(i < 5)
        def _():
            stage_z(i + 3)

        @pl.when(i < 6)
        def _():
            stage_y(i + 2)

        @pl.when(i < 7)
        def _():
            stage_d(i + 1)

        @pl.when(i == 5)
        def _():
            take(ow.at[left], ox_recv.at[0])
            push(ow.at[left, pl.ds(0, 128)], ow.at[left, pl.ds(0, 128)], ox_send.at[3], ox_recv.at[3], at_x(1))
            push(ow.at[left], ow.at[left], ox_send.at[4], ox_recv.at[4], partner)
            take(ow.at[right], ox_recv.at[1])
            push(ow.at[right, pl.ds(128, 128)], ow.at[right, pl.ds(128, 128)], ox_send.at[5], ox_recv.at[5], at_x(-1))
            push(ow.at[right], ow.at[right], ox_send.at[6], ox_recv.at[6], partner)

        at = z_of(i)
        take(kv.at[at, pl.ds(NY * (1 - c), NY)], kd_recv.at[i])
        codes = jnp.concatenate([kv[at, p, 0:PIECE, :] for p in range(2 * NY)], axis=0)
        rot = jnp.concatenate([kv[at, p, PIECE:MSG, 0:PIECE] for p in range(2 * NY)], axis=1)
        keys = lax.dot_general(ket[...], codes, (((1,), (1,)), ((), ())), preferred_element_type=F32).astype(BF16)
        for j in range(2):
            kt2[j, 0:128, :] = keys[128 * j : 128 * (j + 1)]
            for h in range(4):
                kt2[j, 128 + 32 * h : 160 + 32 * h, :] = rot

        def scores(h):
            return dot(q2[h // 2, SLAB * (h % 2) : SLAB * (h % 2 + 1), :], kt2[h // 2])

        coming = scores(0)
        for h in range(4):
            s = coming
            if h < 3:
                coming = scores(h + 1)
            rows = pl.ds(SLAB * h, SLAB)
            old = top[rows, :]
            new = jnp.maximum(old, jnp.max(s, axis=1, keepdims=True))
            w = jnp.exp2(s - new)
            fade = jnp.exp2(old - new)
            top[rows, :] = new
            total[rows, :] = total[rows, :] * fade + jnp.sum(w, axis=1, keepdims=True)
            acc[rows, :] = acc[rows, :] * fade + dot(w.astype(BF16), codes)
        return carry

    lax.fori_loop(0, NZ, one_unit, 0)

    take(ow.at[across, pl.ds(0, 128)], ox_recv.at[3])
    take(ow.at[across, pl.ds(128, 128)], ox_recv.at[5])
    push(ow.at[across], ow.at[across], ox_send.at[7], ox_recv.at[7], partner)

    have(18)
    col = lax.broadcasted_iota(jnp.int32, (SLAB, COL), 1)
    attended = jnp.zeros((SLAB, COL), F32)
    for h in range(4):
        rows = pl.ds(SLAB * h, SLAB)
        inner = (acc[rows, :] / total[rows, :]).astype(BF16)
        attended = jnp.where(col // 64 == h, dot(inner, ve[...]), attended)
    gated = attended * sgate[...]
    for t in range(NTP):
        gsrc[t] = gated[ROWS * t : ROWS * (t + 1), :].astype(BF16)
    gdst[tp] = gsrc[tp]
    for d in range(1, NTP):
        push(gsrc.at[(tp + d) % NTP], gdst.at[tp], a_send.at[d - 1], a_recv.at[d - 1], at_tp(d))

    take(ow.at[partner_slot], ox_recv.at[2])
    for n, d in ((4, -1), (6, 1), (7, 2)):
        take(ow.at[((x + d) % NX) * NC + (1 - c)], ox_recv.at[n])
    for d in range(1, NTP):
        take(gdst.at[(tp - d) % NTP], a_recv.at[d - 1])
    have(20, 21)
    rows_in = jnp.concatenate([gdst[t] for t in range(NTP)], axis=1)
    branch = dot(rows_in, ow[...].reshape(WIDTH, WIDTH))
    blended = SQRT2 * gath[tp].astype(F32) + vector(4) * branch
    centred = blended - jnp.mean(blended, axis=-1, keepdims=True)
    spread = jnp.mean(centred * centred, axis=-1, keepdims=True)
    out[...] = (centred * lax.rsqrt(spread + EPS) * ng[...] + nb[...]).astype(BF16)

    for d in range(NY - 1):
        take(ybuf.at[y], ysend.at[d])
    for d in range(NZ - 1):
        take(zbuf.at[z], zsend.at[d])
    for d in range(NTP - 1):
        take(mod.at[tp], tsend.at[d])
        take(gdst.at[tp], a_send.at[d])
    for n in (0, 1, 2, 4, 6, 7):
        take(gath.at[tp], lx_send.at[n])
        take(ow.at[tp], ox_send.at[n])
    for n in (3, 5):
        take(gath.at[tp, :, first], lx_send.at[n])
        take(ow.at[tp, pl.ds(0, 128)], ox_send.at[n])
    here = kv.at[z, slot]
    for n in range(1, 7):
        take(here, kz_send.at[n])
    take(here.at[low], kz_send.at[7])
    take(here.at[high], kz_send.at[8])

    def drain(i, carry):
        take(here, ky_send.at[i, 0])
        take(here, ky_send.at[i, 1])
        take(here.at[low], ky_send.at[i, 2])
        take(here.at[high], ky_send.at[i, 3])
        take(kv.at[z, pl.ds(0, NY)], kd_send.at[i])
        return carry

    lax.fori_loop(0, NZ, drain, 0)


def per_device(
    latents, context, cond_vec, ctx_vec, shift_w, scale_w, modgate_w, query_down_weight, latent_down_weight, rot_down,
    gate_w, query_norm_gain, latent_norm_gain, query_plain_weight, query_rotary_weight, key_expand_weight,
    value_expand_weight, out_w, norm_gain, norm_bias,
):
    by_slab, by_col = rope_tables()
    args = (
        latents, context, cond_vec.reshape(16, 128), ctx_vec.reshape(16, 128), shift_w, scale_w, modgate_w,
        query_down_weight, latent_down_weight, rot_down, gate_w, query_norm_gain.reshape(1, 512),
        latent_norm_gain.reshape(1, COL), query_plain_weight, query_rotary_weight, key_expand_weight,
        value_expand_weight, out_w, norm_gain.reshape(1, WIDTH), norm_bias.reshape(1, WIDTH),
        jnp.asarray(by_slab), jnp.asarray(by_col),
    )
    vm = pltpu.VMEM
    dma = pltpu.SemaphoreType.DMA
    scratch = [
        vm((NTP, ROWS, WIDTH), BF16), vm((32, WIDTH), BF16), vm((16, 128), F32), vm((16, 128), F32),
        vm((3, 64, COL), BF16), vm((WIDTH, 512), BF16), vm((WIDTH, COL), BF16), vm((WIDTH, 32), BF16),
        vm((WIDTH, COL), BF16), vm((1, 512), F32), vm((1, COL), F32), vm((512, COL), BF16), vm((512, 128), BF16),
        vm((COL, COL), BF16), vm((COL, COL), BF16), vm((NTP, COL, WIDTH), BF16), vm((1, WIDTH), F32),
        vm((1, WIDTH), F32), vm((16, 128), F32), vm((128, 128), F32),
        vm((NY, 8, COL), F32), vm((NZ, 8, COL), F32), vm((NTP, 8, COL), F32), vm((SLAB, WIDTH), BF16),
        vm((32, WIDTH), BF16), vm((SLAB, 128), F32), vm((SLAB, 128), F32), vm((NZ, 2 * NY, MSG, COL), BF16),
        vm((COL, COL), BF16), vm((2, 2 * SLAB, COL), BF16), vm((2, COL, UNIT), BF16), vm((4 * SLAB, COL), F32),
        vm((4 * SLAB, 1), F32), vm((4 * SLAB, 1), F32), vm((SLAB, COL), F32), vm((NTP, ROWS, COL), BF16),
        vm((NTP, ROWS, COL), BF16),
        dma((22,)), dma((NY - 1,)), dma((NY - 1,)), dma((NZ - 1,)), dma((NZ - 1,)), dma((NTP - 1,)), dma((NTP - 1,)),
        dma((8,)), dma((8,)), dma((9,)), dma((9,)), dma((NZ, 4)), dma((NZ, 4)), dma((NZ,)), dma((NZ,)),
        dma((8,)), dma((8,)), dma((NTP - 1,)), dma((NTP - 1,)),
    ]
    return pl.pallas_call(
        body,
        out_shape=jax.ShapeDtypeStruct((ROWS, WIDTH), BF16),
        in_specs=[pl.BlockSpec(memory_space=pl.ANY)] * len(args),
        out_specs=pl.BlockSpec(memory_space=pltpu.VMEM),
        scratch_shapes=scratch,
        compiler_params=pltpu.CompilerParams(collective_id=0, has_side_effects=True, vmem_limit_bytes=62 * 1024 * 1024),
    )(*args)


def solution(mesh):
    tp, sp = P(None, "tp"), P("sp", "tp")
    return jax.shard_map(
        per_device,
        mesh=mesh,
        in_specs=(
            P(("sp", "tp"), None), P("sp", None), P(), P(), sp, sp, sp, P(), P(), P(), tp, P(), P(), tp, tp, tp, tp,
            P("tp", None), P(), P(),
        ),
        out_specs=P(("sp", "tp"), None),
        check_vma=False,
    )
```

```python
import math

import jax
import jax.numpy as jnp
import numpy as np
from jax import lax
from jax.experimental import pallas as pl
from jax.experimental.pallas import tpu as pltpu
from jax.sharding import PartitionSpec as P

F32, BF16 = jnp.float32, jnp.bfloat16
NZ, NY, NX, NC = 8, 4, 4, 2
NTP = NX * NC
NPLANE = NY * NTP
ROWS = 40
SLAB = 320
HALF = 160
CTXH = 16
PIECE = HALF + CTXH
MSG = PIECE + 32
CUT = 112
UNIT = 2 * NY * PIECE
WIDTH = 2048
COL = 256
EPS = 1e-06
OW_MID = 4
SQRT2 = 2.0**0.5
SCORE = math.log2(math.e) / math.sqrt(96.0)


def rope_tables():
    inverse = (10000.0 ** (-np.arange(8, dtype=np.float64) / 8)).astype(np.float32)
    lane = np.arange(128)
    axis, member, pair = (lane // 16) % 2, (lane // 8) % 2, lane % 8
    sign = np.where(member == 0, -1.0, 1.0)

    def rows_of(numbers, which):
        angle = (numbers[:, None].astype(np.float32) * inverse[pair][None, :]).astype(np.float64)
        keep = axis[None, :] == which
        return np.where(keep, np.cos(angle), 0.0), np.where(keep, np.sin(angle) * sign, 0.0)

    cos_row, sin_row = rows_of(np.arange(160), 0)
    cos_col, sin_col = rows_of(np.arange(64), 1)
    by_slab = np.zeros((32, 16, 128), np.float32)
    by_slab[:, 0:5] = cos_row.reshape(32, 5, 128)
    by_slab[:, 8:13] = sin_row.reshape(32, 5, 128)
    return by_slab, np.concatenate([cos_col, sin_col], 0).astype(np.float32)


def dot(a, b):
    return jnp.dot(a, b, preferred_element_type=F32)


def silu(v):
    return v / (1.0 + jnp.exp(-v))


def rms(v, gain):
    return v * lax.rsqrt(jnp.mean(v * v, axis=-1, keepdims=True) + EPS) * gain


def swap_members(v):
    lane = lax.broadcasted_iota(jnp.int32, v.shape, 1)
    return jnp.where(lane % 16 < 8, pltpu.roll(v, 120, 1), pltpu.roll(v, 8, 1))


def body(
    lat_h, ctx_h, cond_h, ctxv_h, shw_h, scw_h, mgw_h, qd_h, ld_h, rd_h, gw_h, qg_h, kg_h, qp_h, qr_h, ke_h, ve_h,
    ow_h, ng_h, nb_h, rrow_h, rcol_h, out,
    gath, ctx_v, cond_v, ctxv_v, w3, qd, ld, rd, gw, qg, kg, qp, qr, ke, ve, ow, ng, nb, rrow, rcol,
    zbuf, pbuf, gbuf, mod, xin, tabc, tabs, kv, ket, q2, kt2, acc, top, total, sgate, gsrc, gdst,
    lsem, zsend, zrecv, psend, precv, gsend, grecv, lx_send, lx_recv, kz_send, kz_recv, ky_send, ky_recv,
    kd_send, kd_recv, kf_send, kf_recv, ox_send, ox_recv, a_send, a_recv,
):
    sp, tp = lax.axis_index("sp"), lax.axis_index("tp")
    z, y, x, c = sp // NY, sp % NY, tp // NC, tp % NC

    def at_z(d):
        return {"sp": ((z + d) % NZ) * NY + y, "tp": tp}

    def at_y(d):
        return {"sp": z * NY + (y + d) % NY, "tp": tp}

    def slot_x(d):
        return ((x + d) % NX) * NC + c

    def at_x(d):
        return {"sp": sp, "tp": slot_x(d)}

    partner_slot = x * NC + (1 - c)
    partner = {"sp": sp, "tp": partner_slot}

    def at_tp(d):
        return {"sp": sp, "tp": (tp + d) % NTP}

    def push(src, dst, send, recv, to):
        pltpu.make_async_remote_copy(
            src_ref=src, dst_ref=dst, send_sem=send, recv_sem=recv, device_id=to, device_id_type=pl.DeviceIdType.MESH
        ).start()

    def take(ref, sem):
        pltpu.make_async_copy(ref, ref, sem).wait()

    local = [
        (cond_h, cond_v), (ctxv_h, ctxv_v), (shw_h, w3.at[0]), (scw_h, w3.at[1]), (mgw_h, w3.at[2]),
        (lat_h, gath.at[tp]), (ctx_h, ctx_v), (ld_h, ld), (rd_h, rd), (rrow_h.at[sp], rrow), (rcol_h, rcol),
        (kg_h, kg), (qd_h, qd), (qg_h, qg), (qp_h, qp), (qr_h, qr), (gw_h, gw), (ke_h, ke), (ve_h, ve),
        (ow_h, ow.at[tp]), (ng_h, ng), (nb_h, nb),
    ]
    for k, (src, dst) in enumerate(local):
        pltpu.make_async_copy(src, dst, lsem.at[k]).start()

    def have(*which):
        for k in which:
            take(local[k][1], lsem.at[k])

    barrier = pltpu.get_barrier_semaphore()
    plane = [(dy, dt) for dy in range(NY) for dt in range(NTP) if (dy, dt) != (0, 0)]

    def at_plane(dy, dt):
        return {"sp": z * NY + (y + dy) % NY, "tp": (tp + dt) % NTP}

    peers = [at_z(d) for d in range(1, NZ)] + [at_plane(dy, dt) for dy, dt in plane]
    for peer in peers:
        pl.semaphore_signal(barrier, inc=1, device_id=peer, device_id_type=pl.DeviceIdType.MESH)

    have(0, 1, 2, 3, 4)
    pick = pl.ds(sp // 2, 1)
    lane = lax.broadcasted_iota(jnp.int32, (8, 128), 1)
    line = lax.broadcasted_iota(jnp.int32, (8, 128), 0)
    mine = lane // 64 == sp % 2
    cond_row = jnp.broadcast_to(silu(cond_v[pick, :]), (8, 128))
    ctxv_row = jnp.broadcast_to(silu(ctxv_v[pick, :]), (8, 128))
    part = jnp.zeros((8, COL), F32)
    for k in range(3):
        at = 2 * k
        rows = jnp.where(line == at, cond_row, jnp.where(line == at + 1, ctxv_row, 0.0))
        rows = jnp.where(mine, rows, 0.0).astype(BF16)
        part = part + dot(rows, jnp.concatenate([w3[k], w3[k]], axis=0))
    zbuf[z] = jnp.concatenate([part[0:4, 0:128], part[0:4, 128:256], part[4:8, 0:128], part[4:8, 128:256]], axis=0)
    pl.semaphore_wait(barrier, len(peers))

    for d in range(1, NZ):
        push(zbuf.at[z], zbuf.at[z], zsend, zrecv, at_z(d))
    have(5)
    own = gath.at[tp]
    push(own, own, lx_send.at[0], lx_recv.at[0], at_x(1))
    push(own, own, lx_send.at[1], lx_recv.at[1], at_x(-1))
    push(own, own, lx_send.at[2], lx_recv.at[2], partner)
    take(zbuf.at[pl.ds(0, NZ - 1)], zrecv)
    whole = zbuf[0]
    for k in range(1, NZ):
        whole = whole + zbuf[k]
    me = y * NTP + tp
    pbuf[me] = whole[0:8]
    gbuf[me] = whole[8:16]
    for dy, dt in plane:
        push(pbuf.at[me], pbuf.at[me], psend, precv, at_plane(dy, dt))

    left, right, across = slot_x(-1), slot_x(1), slot_x(2)
    first, second = pl.ds(0, WIDTH // 2), pl.ds(WIDTH // 2, WIDTH // 2)
    take(gath.at[left], lx_recv.at[0])
    push(gath.at[left, :, first], gath.at[left, :, first], lx_send.at[3], lx_recv.at[3], at_x(1))
    push(gath.at[left], gath.at[left], lx_send.at[4], lx_recv.at[4], partner)
    take(gath.at[right], lx_recv.at[1])
    push(gath.at[right, :, second], gath.at[right, :, second], lx_send.at[5], lx_recv.at[5], at_x(-1))
    push(gath.at[right], gath.at[right], lx_send.at[6], lx_recv.at[6], partner)

    def gate_to_plane():
        for dy, dt in plane:
            push(gbuf.at[me], gbuf.at[me], gsend, grecv, at_plane(dy, dt))

    have(9, 10, 17)
    for k in range(5):
        rows = pl.ds(64 * k, 64)
        tabc[rows, :] = rrow[k : k + 1, :] + rcol[0:64, :]
        tabs[rows, :] = rrow[8 + k : 9 + k, :] + rcol[64:128, :]
    ket[...] = ke[...].astype(F32).T.astype(BF16)
    top[...] = jnp.full(top.shape, -1e30, F32)
    total[...] = jnp.zeros(total.shape, F32)
    acc[...] = jnp.zeros(acc.shape, F32)

    take(gath.at[across, :, first], lx_recv.at[3])
    take(gath.at[across, :, second], lx_recv.at[5])
    push(gath.at[across], gath.at[across], lx_send.at[7], lx_recv.at[7], partner)

    def from_plane(buf, sem):
        take(buf.at[pl.ds(0, NPLANE - 1)], sem)
        for t in range(NTP):
            mod[t] = (buf[t] + buf[NTP + t]) + (buf[2 * NTP + t] + buf[3 * NTP + t])

    from_plane(pbuf, precv)
    def vector(row):
        return jnp.concatenate([mod[t, r : r + 1, :] for t in range(NTP) for r in (row, row + 4)], axis=1)

    shift, scale = vector(0), 1.0 + vector(2)
    have(6, 7, 8, 11)
    lines = [gath[NC * k + c].astype(F32) for k in range(NX)]
    mine_lat = jnp.concatenate(lines, axis=0) * scale + shift
    mine_ctx = ctx_v[pl.ds(pl.multiple_of(CTXH * c, CTXH), CTXH), :].astype(F32) * (1.0 + vector(3)) + vector(1)
    mine_in = jnp.concatenate([mine_lat, mine_ctx], axis=0).astype(BF16)
    slot = NY * c + y
    kv[z, slot, 0:PIECE, :] = rms(dot(mine_in, ld[...]), kg[...]).astype(BF16)
    flat = lax.dot_general(mine_in, rd[...], (((1,), (1,)), ((), ())), preferred_element_type=F32)
    flat = jnp.concatenate([flat, jnp.zeros((PIECE, 96), F32)], axis=1)
    lat_part = flat[0:HALF]

    def rows_of(table):
        return jnp.concatenate(
            [table[pl.ds(pl.multiple_of(ROWS * (NC * k + c), 8), ROWS), :] for k in range(NX)], axis=0
        )

    turned = lat_part * rows_of(tabc) + swap_members(lat_part) * rows_of(tabs)
    both = jnp.concatenate([turned, flat[HALF:], jnp.zeros((256 - PIECE, 128), F32)], axis=0)
    kv[z, slot, PIECE:MSG, :] = both.T[0:32, :].astype(BF16)

    def z_of(i):
        off = (i % 2) * ((i + 1) // 2) - (1 - i % 2) * (i // 2)
        return (z + off + NZ) % NZ

    low, high = pl.ds(0, CUT), pl.ds(CUT, MSG - CUT)

    def z_back(i):
        return {"sp": ((z + NZ + 1 - 2 * (i % 2)) % NZ) * NY + y, "tp": tp}

    def at_slot(i, d):
        return kv.at[z_of(i), NY * c + (y + d + NY) % NY]

    def near_z(i):
        here = at_slot(i, 0)

        @pl.when(i < 7)
        def _():
            take(here, kz_recv.at[i, 0])

        @pl.when(i == 7)
        def _():
            take(here.at[low], kz_recv.at[7, 0])
            take(here.at[high], kz_recv.at[7, 1])

        @pl.when(i < 5)
        def _():
            push(here, here, kz_send.at[i + 2, 0], kz_recv.at[i + 2, 0], z_back(i))

        @pl.when(i == 5)
        def _():
            push(here.at[low], here.at[low], kz_send.at[7, 0], kz_recv.at[7, 0], at_z(-1))

        @pl.when(i == 6)
        def _():
            push(here.at[high], here.at[high], kz_send.at[7, 1], kz_recv.at[7, 1], at_z(1))

        to_y(i)

    def to_y(i):
        here = at_slot(i, 0)
        push(here, here, ky_send.at[i, 0], ky_recv.at[i, 0], at_y(1))
        push(here, here, ky_send.at[i, 1], ky_recv.at[i, 1], at_y(-1))

    def from_y(i):
        below, above = at_slot(i, -1), at_slot(i, 1)
        take(below, ky_recv.at[i, 0])
        push(below.at[low], below.at[low], ky_send.at[i, 2], ky_recv.at[i, 2], at_y(1))
        take(above, ky_recv.at[i, 1])
        push(above.at[high], above.at[high], ky_send.at[i, 3], ky_recv.at[i, 3], at_y(-1))

    def from_far(i):
        far = at_slot(i, 2)
        take(far.at[low], ky_recv.at[i, 2])
        take(far.at[high], ky_recv.at[i, 3])

    def to_partner(i):
        four = kv.at[z_of(i), pl.ds(NY * c, NY)]
        push(four, four, kd_send.at[i], kd_recv.at[i], partner)

    turn = (0, 1, -1, 2)

    def own_to_z(j):
        here = at_slot(0, turn[j])
        push(here, here, kz_send.at[1, j], kz_recv.at[1, j], at_z(-1))
        push(here, here, kz_send.at[2, j], kz_recv.at[2, j], at_z(1))

    def round_z(i):
        for j in range(4):
            here = at_slot(i, turn[j])
            take(here, kz_recv.at[i, j])

            @pl.when((i < 5) | ((i == 5) & (j < 2)) | ((i == 6) & (j >= 2)))
            def _(here=here, j=j):
                n = jnp.minimum(i + 2, 7)
                push(here, here, kz_send.at[n, j], kz_recv.at[n, j], z_back(i))

    first_y = kv.at[z, slot]
    push(first_y.at[low], first_y.at[low], kf_send.at[0], kf_recv.at[0], at_y(1))
    push(first_y.at[high], first_y.at[high], kf_send.at[1], kf_recv.at[1], at_y(-1))
    push(first_y.at[high], first_y.at[high], kf_send.at[2], kf_recv.at[2], at_y(1))
    push(first_y.at[low], first_y.at[low], kf_send.at[3], kf_recv.at[3], at_y(-1))
    own_to_z(0)
    have(19)
    owned = ow.at[tp]
    push(owned, owned, ox_send.at[0], ox_recv.at[0], at_x(1))
    push(owned, owned, ox_send.at[1], ox_recv.at[1], at_x(-1))
    push(owned, owned, ox_send.at[2], ox_recv.at[2], partner)

    take(gath.at[partner_slot], lx_recv.at[2])
    for n, d in ((4, -1), (6, 1), (7, 2)):
        take(gath.at[((x + d) % NX) * NC + (1 - c)], lx_recv.at[n])
    for p in range(NTP // 2):
        pair = jnp.concatenate([gath[2 * p].astype(F32), gath[2 * p + 1].astype(F32)], axis=0)
        xin[2 * ROWS * p : 2 * ROWS * (p + 1), :] = (pair * scale + shift).astype(BF16)

    have(12, 13, 14, 15)
    q_codes = rms(dot(xin[...], qd[...]), qg[...]).astype(BF16)
    q_cont = dot(q_codes, qp[...]) * SCORE
    q_rot = dot(q_codes, qr[...])
    q_rot = (q_rot * tabc[...] + swap_members(q_rot) * tabs[...]) * SCORE
    q_lane = lax.broadcasted_iota(jnp.int32, (SLAB, 128), 1)
    for h in range(4):
        j, rows = h // 2, pl.ds(SLAB * (h % 2), SLAB)
        plain = q_cont[:, 128 * j : 128 * (j + 1)]
        q2[j, rows, 0:128] = jnp.where(q_lane // 64 == h % 2, plain, 0.0).astype(BF16)
        q2[j, rows, 128:256] = jnp.where(q_lane // 32 == h, q_rot, 0.0).astype(BF16)
    below, above = at_slot(0, -1), at_slot(0, 1)
    take(below.at[low], kf_recv.at[0])
    push(below.at[low], below.at[low], ky_send.at[0, 2], ky_recv.at[0, 2], at_y(1))
    take(above.at[high], kf_recv.at[1])
    push(above.at[high], above.at[high], ky_send.at[0, 3], ky_recv.at[0, 3], at_y(-1))

    @pl.when(c == 0)
    def _():
        near_z(1)
        near_z(2)

    take(below.at[high], kf_recv.at[2])
    take(above.at[low], kf_recv.at[3])

    @pl.when(c == 1)
    def _():
        own_to_z(1)
        own_to_z(2)

    have(16)
    sgate[...] = silu(dot(xin[...], gw[...]).astype(BF16).astype(F32))
    from_far(0)
    to_partner(0)

    @pl.when(c == 0)
    def _():
        from_y(1)

    @pl.when(c == 1)
    def _():
        own_to_z(3)

    def halfway(i):
        @pl.when((c == 1) & (i % 2 == 0))
        def _():
            round_z(i + 1)

        @pl.when((c == 1) & (i % 2 == 0) & (i < 6))
        def _():
            round_z(i + 2)

        @pl.when((c == 0) & (i < 7))
        def _():
            from_far(i + 1)

        @pl.when(i < 7)
        def _():
            to_partner(i + 1)

    def one_unit(i, carry):
        @pl.when((c == 0) & (i < 5))
        def _():
            near_z(i + 3)

        @pl.when((c == 0) & (i < 6))
        def _():
            from_y(i + 2)

        @pl.when(i == 1)
        def _():
            gate_to_plane()

        @pl.when(i == OW_MID)
        def _():
            take(ow.at[left], ox_recv.at[0])
            push(ow.at[left, pl.ds(0, 128)], ow.at[left, pl.ds(0, 128)], ox_send.at[3], ox_recv.at[3], at_x(1))
            push(ow.at[left], ow.at[left], ox_send.at[4], ox_recv.at[4], partner)
            take(ow.at[right], ox_recv.at[1])
            push(ow.at[right, pl.ds(128, 128)], ow.at[right, pl.ds(128, 128)], ox_send.at[5], ox_recv.at[5], at_x(-1))
            push(ow.at[right], ow.at[right], ox_send.at[6], ox_recv.at[6], partner)

        @pl.when(i == 7)
        def _():
            take(ow.at[across, pl.ds(0, 128)], ox_recv.at[3])
            take(ow.at[across, pl.ds(128, 128)], ox_recv.at[5])
            push(ow.at[across], ow.at[across], ox_send.at[7], ox_recv.at[7], partner)

        at = z_of(i)
        take(kv.at[at, pl.ds(NY * (1 - c), NY)], kd_recv.at[i])
        codes = jnp.concatenate([kv[at, p, 0:PIECE, :] for p in range(2 * NY)], axis=0)
        rot = jnp.concatenate([kv[at, p, PIECE:MSG, 0:PIECE] for p in range(2 * NY)], axis=1)
        keys = lax.dot_general(ket[...], codes, (((1,), (1,)), ((), ())), preferred_element_type=F32).astype(BF16)
        for j in range(2):
            kt2[j, 0:128, :] = keys[128 * j : 128 * (j + 1)]
            for h in range(4):
                kt2[j, 128 + 32 * h : 160 + 32 * h, :] = rot

        def scores(h):
            return dot(q2[h // 2, SLAB * (h % 2) : SLAB * (h % 2 + 1), :], kt2[h // 2])

        coming = scores(0)
        for h in range(4):
            s = coming
            if h == 2:
                halfway(i)
            if h < 3:
                coming = scores(h + 1)
            rows = pl.ds(SLAB * h, SLAB)
            old = top[rows, :]
            new = jnp.maximum(old, jnp.max(s, axis=1, keepdims=True))
            w = jnp.exp2(s - new)
            fade = jnp.exp2(old - new)
            top[rows, :] = new
            total[rows, :] = total[rows, :] * fade + jnp.sum(w, axis=1, keepdims=True)
            acc[rows, :] = acc[rows, :] * fade + dot(w.astype(BF16), codes)
        return carry

    lax.fori_loop(0, NZ, one_unit, 0)

    have(18)
    col = lax.broadcasted_iota(jnp.int32, (SLAB, COL), 1)
    attended = jnp.zeros((SLAB, COL), F32)
    for h in range(4):
        rows = pl.ds(SLAB * h, SLAB)
        inner = (acc[rows, :] / total[rows, :]).astype(BF16)
        attended = jnp.where(col // 64 == h, dot(inner, ve[...]), attended)
    gated = attended * sgate[...]
    for t in range(NTP):
        gsrc[t] = gated[ROWS * t : ROWS * (t + 1), :].astype(BF16)
    gdst[tp] = gsrc[tp]
    sources = (1, 7, 2, 6, 3, 5, 4)
    for n, d in enumerate(sources):
        push(gsrc.at[(tp + d) % NTP], gdst.at[tp], a_send, a_recv.at[n], at_tp(d))

    have(20, 21)
    from_plane(gbuf, grecv)
    take(zbuf.at[pl.ds(0, NZ - 1)], zsend)
    take(pbuf.at[pl.ds(0, NPLANE - 1)], psend)
    take(gbuf.at[pl.ds(0, NPLANE - 1)], gsend)
    for n in (0, 1, 2, 4, 6, 7):
        take(gath.at[tp], lx_send.at[n])
        take(ow.at[tp], ox_send.at[n])
    for n in (3, 5):
        take(gath.at[tp, :, first], lx_send.at[n])
        take(ow.at[tp, pl.ds(0, 128)], ox_send.at[n])
    here = kv.at[z, slot]

    def sent_along_y(i):
        take(here, ky_send.at[i, 0])
        take(here, ky_send.at[i, 1])
        take(here.at[low], ky_send.at[i, 2])
        take(here.at[high], ky_send.at[i, 3])

    take(here.at[low], kf_send.at[0])
    take(here.at[high], kf_send.at[1])
    take(here.at[high], kf_send.at[2])
    take(here.at[low], kf_send.at[3])
    take(here.at[low], ky_send.at[0, 2])
    take(here.at[high], ky_send.at[0, 3])
    take(kv.at[z, pl.ds(0, NY)], kd_send.at[0])

    def drain(i, carry):
        take(kv.at[z, pl.ds(0, NY)], kd_send.at[i])

        @pl.when(c == 0)
        def _():
            sent_along_y(i)

        @pl.when((c == 1) | (i < 7))
        def _():
            take(here, kz_send.at[i, 0])

        @pl.when(c == 1)
        def _():
            for j in range(1, 4):
                take(here, kz_send.at[i, j])

        return carry

    lax.fori_loop(1, NZ, drain, 0)

    @pl.when(c == 0)
    def _():
        take(here.at[low], kz_send.at[7, 0])
        take(here.at[high], kz_send.at[7, 1])

    take(ow.at[partner_slot], ox_recv.at[2])
    for n, d in ((4, -1), (6, 1), (7, 2)):
        take(ow.at[((x + d) % NX) * NC + (1 - c)], ox_recv.at[n])
    outer = dot(gdst[tp], ow[tp])
    for n, d in enumerate(sources):
        src = (tp - d) % NTP
        take(gdst.at[src], a_recv.at[n])
        outer = outer + dot(gdst[src], ow[src])
    blended = SQRT2 * gath[tp].astype(F32) + vector(0) * outer
    centred = blended - jnp.mean(blended, axis=-1, keepdims=True)
    spread = jnp.mean(centred * centred, axis=-1, keepdims=True)
    out[...] = (centred * lax.rsqrt(spread + EPS) * ng[...] + nb[...]).astype(BF16)
    take(gsrc.at[pl.ds(0, NTP - 1)], a_send)


def per_device(
    latents, context, cond_vec, ctx_vec, shift_w, scale_w, modgate_w, query_down_weight, latent_down_weight, rot_down,
    gate_w, query_norm_gain, latent_norm_gain, query_plain_weight, query_rotary_weight, key_expand_weight,
    value_expand_weight, out_w, norm_gain, norm_bias,
):
    by_slab, by_col = rope_tables()
    args = (
        latents, context, cond_vec.reshape(16, 128), ctx_vec.reshape(16, 128), shift_w, scale_w, modgate_w,
        query_down_weight, latent_down_weight, rot_down.T, gate_w, query_norm_gain.reshape(1, 512),
        latent_norm_gain.reshape(1, COL), query_plain_weight, query_rotary_weight, key_expand_weight,
        value_expand_weight, out_w, norm_gain.reshape(1, WIDTH), norm_bias.reshape(1, WIDTH),
        jnp.asarray(by_slab), jnp.asarray(by_col),
    )
    vm = pltpu.VMEM
    dma = pltpu.SemaphoreType.DMA
    scratch = [
        vm((NTP, ROWS, WIDTH), BF16), vm((32, WIDTH), BF16), vm((16, 128), F32), vm((16, 128), F32),
        vm((3, 64, COL), BF16), vm((WIDTH, 512), BF16), vm((WIDTH, COL), BF16), vm((32, WIDTH), BF16),
        vm((WIDTH, COL), BF16), vm((1, 512), F32), vm((1, COL), F32), vm((512, COL), BF16), vm((512, 128), BF16),
        vm((COL, COL), BF16), vm((COL, COL), BF16), vm((NTP, COL, WIDTH), BF16), vm((1, WIDTH), F32),
        vm((1, WIDTH), F32), vm((16, 128), F32), vm((128, 128), F32),
        vm((NZ, 16, 128), F32), vm((NPLANE, 8, 128), F32), vm((NPLANE, 8, 128), F32), vm((NTP, 8, 128), F32),
        vm((SLAB, WIDTH), BF16),
        vm((SLAB, 128), F32), vm((SLAB, 128), F32), vm((NZ, 2 * NY, MSG, COL), BF16),
        vm((COL, COL), BF16), vm((2, 2 * SLAB, COL), BF16), vm((2, COL, UNIT), BF16), vm((4 * SLAB, COL), F32),
        vm((4 * SLAB, 1), F32), vm((4 * SLAB, 1), F32), vm((SLAB, COL), F32), vm((NTP, ROWS, COL), BF16),
        vm((NTP, ROWS, COL), BF16),
        dma((22,)), dma, dma, dma, dma, dma, dma,
        dma((8,)), dma((8,)), dma((NZ, 4)), dma((NZ, 4)), dma((NZ, 4)), dma((NZ, 4)), dma((NZ,)), dma((NZ,)), dma((4,)), dma((4,)),
        dma((8,)), dma((8,)), dma, dma((NTP - 1,)),
    ]
    return pl.pallas_call(
        body,
        out_shape=jax.ShapeDtypeStruct((ROWS, WIDTH), BF16),
        in_specs=[pl.BlockSpec(memory_space=pl.ANY)] * len(args),
        out_specs=pl.BlockSpec(memory_space=pltpu.VMEM),
        scratch_shapes=scratch,
        compiler_params=pltpu.CompilerParams(collective_id=0, has_side_effects=True, vmem_limit_bytes=62 * 1024 * 1024),
    )(*args)


def solution(mesh):
    tp, sp = P(None, "tp"), P("sp", "tp")
    return jax.shard_map(
        per_device,
        mesh=mesh,
        in_specs=(
            P(("sp", "tp"), None), P("sp", None), P(), P(), sp, sp, sp, P(), P(), P(), tp, P(), P(), tp, tp, tp, tp,
            P("tp", None), P(), P(),
        ),
        out_specs=P(("sp", "tp"), None),
        check_vma=False,
    )
```

```python
import math

import jax
import jax.numpy as jnp
import numpy as np
from jax import lax
from jax.experimental import pallas as pl
from jax.experimental.pallas import tpu as pltpu
from jax.sharding import PartitionSpec as P

F32, BF16 = jnp.float32, jnp.bfloat16
NZ, NY, NX, NC = 8, 4, 4, 2
NTP = NX * NC
NPLANE = NY * NTP
ROWS = 40
SLAB = 320
HALF = 160
CTXH = 16
PIECE = HALF + CTXH
MSG = PIECE + 32
CUT = 112
UNIT = 2 * NY * PIECE
WIDTH = 2048
COL = 256
EPS = 1e-06
OW_MID = 4
SQRT2 = 2.0**0.5
SCORE = math.log2(math.e) / math.sqrt(96.0)


def rope_tables():
    inverse = (10000.0 ** (-np.arange(8, dtype=np.float64) / 8)).astype(np.float32)
    lane = np.arange(128)
    axis, member, pair = (lane // 16) % 2, (lane // 8) % 2, lane % 8
    sign = np.where(member == 0, -1.0, 1.0)

    def rows_of(numbers, which):
        angle = (numbers[:, None].astype(np.float32) * inverse[pair][None, :]).astype(np.float64)
        keep = axis[None, :] == which
        return np.where(keep, np.cos(angle), 0.0), np.where(keep, np.sin(angle) * sign, 0.0)

    cos_row, sin_row = rows_of(np.arange(160), 0)
    cos_col, sin_col = rows_of(np.arange(64), 1)
    by_slab = np.zeros((32, 16, 128), np.float32)
    by_slab[:, 0:5] = cos_row.reshape(32, 5, 128)
    by_slab[:, 8:13] = sin_row.reshape(32, 5, 128)
    return by_slab, np.concatenate([cos_col, sin_col], 0).astype(np.float32)


def dot(a, b):
    return jnp.dot(a, b, preferred_element_type=F32)


def silu(v):
    return v / (1.0 + jnp.exp(-v))


def rms(v, gain):
    return v * lax.rsqrt(jnp.mean(v * v, axis=-1, keepdims=True) + EPS) * gain


def swap_members(v):
    lane = lax.broadcasted_iota(jnp.int32, v.shape, 1)
    return jnp.where(lane % 16 < 8, pltpu.roll(v, 120, 1), pltpu.roll(v, 8, 1))


def body(
    lat_h, ctx_h, cond_h, ctxv_h, shw_h, scw_h, mgw_h, qd_h, ld_h, rd_h, gw_h, qg_h, kg_h, qp_h, qr_h, ke_h, ve_h,
    ow_h, ng_h, nb_h, rrow_h, rcol_h, out,
    gath, ctx_v, cond_v, ctxv_v, w3, qd, ld, rd, gw, qg, kg, qp, qr, ke, ve, ow, ng, nb, rrow, rcol,
    zbuf, pbuf, gbuf, mod, xin, tabc, tabs, kv, ket, q2, kt2, acc, top, total, sgate, gsrc, gdst,
    lsem, zsend, zrecv, psend, precv, gsend, grecv, lx_send, lx_recv, kz_send, kz_recv, ky_send, ky_recv,
    kd_send, kd_recv, kf_send, kf_recv, ox_send, ox_recv, a_send, a_recv,
):
    sp, tp = lax.axis_index("sp"), lax.axis_index("tp")
    z, y, x, c = sp // NY, sp % NY, tp // NC, tp % NC

    def at_z(d):
        return {"sp": ((z + d) % NZ) * NY + y, "tp": tp}

    def at_y(d):
        return {"sp": z * NY + (y + d) % NY, "tp": tp}

    def slot_x(d):
        return ((x + d) % NX) * NC + c

    def at_x(d):
        return {"sp": sp, "tp": slot_x(d)}

    partner_slot = x * NC + (1 - c)
    partner = {"sp": sp, "tp": partner_slot}

    def at_tp(d):
        return {"sp": sp, "tp": (tp + d) % NTP}

    def push(src, dst, send, recv, to):
        pltpu.make_async_remote_copy(
            src_ref=src, dst_ref=dst, send_sem=send, recv_sem=recv, device_id=to, device_id_type=pl.DeviceIdType.MESH
        ).start()

    def take(ref, sem):
        pltpu.make_async_copy(ref, ref, sem).wait()

    local = [
        (cond_h, cond_v), (ctxv_h, ctxv_v), (shw_h, w3.at[0]), (scw_h, w3.at[1]), (mgw_h, w3.at[2]),
        (lat_h, gath.at[tp]), (ctx_h, ctx_v), (ld_h, ld), (rd_h, rd), (rrow_h.at[sp], rrow), (rcol_h, rcol),
        (kg_h, kg), (qd_h, qd), (qg_h, qg), (qp_h, qp), (qr_h, qr), (gw_h, gw), (ke_h, ke), (ve_h, ve),
        (ow_h, ow.at[tp]), (ng_h, ng), (nb_h, nb),
    ]
    for k, (src, dst) in enumerate(local):
        pltpu.make_async_copy(src, dst, lsem.at[k]).start()

    def have(*which):
        for k in which:
            take(local[k][1], lsem.at[k])

    barrier = pltpu.get_barrier_semaphore()
    plane = [(dy, dt) for dy in range(NY) for dt in range(NTP) if (dy, dt) != (0, 0)]

    def at_plane(dy, dt):
        return {"sp": z * NY + (y + dy) % NY, "tp": (tp + dt) % NTP}

    peers = [at_z(d) for d in range(1, NZ)] + [at_plane(dy, dt) for dy, dt in plane]
    for peer in peers:
        pl.semaphore_signal(barrier, inc=1, device_id=peer, device_id_type=pl.DeviceIdType.MESH)

    have(0, 1, 2, 3, 4)
    pick = pl.ds(sp // 2, 1)
    lane = lax.broadcasted_iota(jnp.int32, (8, 128), 1)
    line = lax.broadcasted_iota(jnp.int32, (8, 128), 0)
    mine = lane // 64 == sp % 2
    cond_row = jnp.broadcast_to(silu(cond_v[pick, :]), (8, 128))
    ctxv_row = jnp.broadcast_to(silu(ctxv_v[pick, :]), (8, 128))
    part = jnp.zeros((8, COL), F32)
    for k in range(3):
        at = 2 * k
        rows = jnp.where(line == at, cond_row, jnp.where(line == at + 1, ctxv_row, 0.0))
        rows = jnp.where(mine, rows, 0.0).astype(BF16)
        part = part + dot(rows, jnp.concatenate([w3[k], w3[k]], axis=0))
    zbuf[z] = jnp.concatenate([part[0:4, 0:128], part[0:4, 128:256], part[4:8, 0:128], part[4:8, 128:256]], axis=0)
    pl.semaphore_wait(barrier, len(peers))

    for d in range(1, NZ):
        push(zbuf.at[z], zbuf.at[z], zsend, zrecv, at_z(d))
    have(5)
    own = gath.at[tp]
    push(own, own, lx_send.at[0], lx_recv.at[0], at_x(1))
    push(own, own, lx_send.at[1], lx_recv.at[1], at_x(-1))
    push(own, own, lx_send.at[2], lx_recv.at[2], partner)
    take(zbuf.at[pl.ds(0, NZ - 1)], zrecv)
    whole = zbuf[0]
    for k in range(1, NZ):
        whole = whole + zbuf[k]
    me = y * NTP + tp
    pbuf[me] = whole[0:8]
    gbuf[me] = whole[8:16]
    for dy, dt in plane:
        push(pbuf.at[me], pbuf.at[me], psend, precv, at_plane(dy, dt))

    left, right, across = slot_x(-1), slot_x(1), slot_x(2)
    first, second = pl.ds(0, WIDTH // 2), pl.ds(WIDTH // 2, WIDTH // 2)
    take(gath.at[left], lx_recv.at[0])
    push(gath.at[left, :, first], gath.at[left, :, first], lx_send.at[3], lx_recv.at[3], at_x(1))
    push(gath.at[left], gath.at[left], lx_send.at[4], lx_recv.at[4], partner)
    take(gath.at[right], lx_recv.at[1])
    push(gath.at[right, :, second], gath.at[right, :, second], lx_send.at[5], lx_recv.at[5], at_x(-1))
    push(gath.at[right], gath.at[right], lx_send.at[6], lx_recv.at[6], partner)

    def gate_to_plane():
        for dy, dt in plane:
            push(gbuf.at[me], gbuf.at[me], gsend, grecv, at_plane(dy, dt))

    have(9, 10, 17)
    for k in range(5):
        rows = pl.ds(64 * k, 64)
        tabc[rows, :] = rrow[k : k + 1, :] + rcol[0:64, :]
        tabs[rows, :] = rrow[8 + k : 9 + k, :] + rcol[64:128, :]
    ket[...] = ke[...].astype(F32).T.astype(BF16)
    top[...] = jnp.full(top.shape, -1e30, F32)
    total[...] = jnp.zeros(total.shape, F32)
    acc[...] = jnp.zeros(acc.shape, F32)

    take(gath.at[across, :, first], lx_recv.at[3])
    take(gath.at[across, :, second], lx_recv.at[5])
    push(gath.at[across], gath.at[across], lx_send.at[7], lx_recv.at[7], partner)

    def from_plane(buf, sem):
        take(buf.at[pl.ds(0, NPLANE - 1)], sem)
        for t in range(NTP):
            mod[t] = (buf[t] + buf[NTP + t]) + (buf[2 * NTP + t] + buf[3 * NTP + t])

    from_plane(pbuf, precv)
    def vector(row):
        return jnp.concatenate([mod[t, r : r + 1, :] for t in range(NTP) for r in (row, row + 4)], axis=1)

    shift, scale = vector(0), 1.0 + vector(2)
    have(6, 7, 8, 11)
    lines = [gath[NC * k + c].astype(F32) for k in range(NX)]
    mine_lat = jnp.concatenate(lines, axis=0) * scale + shift
    mine_ctx = ctx_v[pl.ds(pl.multiple_of(CTXH * c, CTXH), CTXH), :].astype(F32) * (1.0 + vector(3)) + vector(1)
    mine_in = jnp.concatenate([mine_lat, mine_ctx], axis=0).astype(BF16)
    slot = NY * c + y
    kv[z, slot, 0:PIECE, :] = rms(dot(mine_in, ld[...]), kg[...]).astype(BF16)
    flat = lax.dot_general(mine_in, rd[...], (((1,), (1,)), ((), ())), preferred_element_type=F32)
    flat = jnp.concatenate([flat, jnp.zeros((PIECE, 96), F32)], axis=1)
    lat_part = flat[0:HALF]

    def rows_of(table):
        return jnp.concatenate(
            [table[pl.ds(pl.multiple_of(ROWS * (NC * k + c), 8), ROWS), :] for k in range(NX)], axis=0
        )

    turned = lat_part * rows_of(tabc) + swap_members(lat_part) * rows_of(tabs)
    both = jnp.concatenate([turned, flat[HALF:], jnp.zeros((256 - PIECE, 128), F32)], axis=0)
    kv[z, slot, PIECE:MSG, :] = both.T[0:32, :].astype(BF16)

    def z_of(i):
        off = (i % 2) * ((i + 1) // 2) - (1 - i % 2) * (i // 2)
        return (z + off + NZ) % NZ

    low, high = pl.ds(0, CUT), pl.ds(CUT, MSG - CUT)

    def z_back(i):
        return {"sp": ((z + NZ + 1 - 2 * (i % 2)) % NZ) * NY + y, "tp": tp}

    def at_slot(i, d):
        return kv.at[z_of(i), NY * c + (y + d + NY) % NY]

    def near_z(i):
        here = at_slot(i, 0)

        @pl.when(i < 7)
        def _():
            take(here, kz_recv.at[i, 0])

        @pl.when(i == 7)
        def _():
            take(here.at[low], kz_recv.at[7, 0])
            take(here.at[high], kz_recv.at[7, 1])

        @pl.when(i < 5)
        def _():
            push(here, here, kz_send.at[i + 2, 0], kz_recv.at[i + 2, 0], z_back(i))

        @pl.when(i == 5)
        def _():
            push(here.at[low], here.at[low], kz_send.at[7, 0], kz_recv.at[7, 0], at_z(-1))

        @pl.when(i == 6)
        def _():
            push(here.at[high], here.at[high], kz_send.at[7, 1], kz_recv.at[7, 1], at_z(1))

        to_y(i)

    def to_y(i):
        here = at_slot(i, 0)
        push(here, here, ky_send.at[i, 0], ky_recv.at[i, 0], at_y(1))
        push(here, here, ky_send.at[i, 1], ky_recv.at[i, 1], at_y(-1))

    def from_y(i):
        below, above = at_slot(i, -1), at_slot(i, 1)
        take(below, ky_recv.at[i, 0])
        push(below.at[low], below.at[low], ky_send.at[i, 2], ky_recv.at[i, 2], at_y(1))
        take(above, ky_recv.at[i, 1])
        push(above.at[high], above.at[high], ky_send.at[i, 3], ky_recv.at[i, 3], at_y(-1))

    def from_far(i):
        far = at_slot(i, 2)
        take(far.at[low], ky_recv.at[i, 2])
        take(far.at[high], ky_recv.at[i, 3])

    def to_partner(i):
        four = kv.at[z_of(i), pl.ds(NY * c, NY)]
        push(four, four, kd_send.at[i], kd_recv.at[i], partner)

    turn = (0, 1, -1, 2)

    def own_to_z(j):
        here = at_slot(0, turn[j])
        push(here, here, kz_send.at[1, j], kz_recv.at[1, j], at_z(-1))
        push(here, here, kz_send.at[2, j], kz_recv.at[2, j], at_z(1))

    def round_z(i):
        for j in range(4):
            here = at_slot(i, turn[j])
            take(here, kz_recv.at[i, j])

            @pl.when((i < 5) | ((i == 5) & (j < 2)) | ((i == 6) & (j >= 2)))
            def _(here=here, j=j):
                n = jnp.minimum(i + 2, 7)
                push(here, here, kz_send.at[n, j], kz_recv.at[n, j], z_back(i))

    first_y = kv.at[z, slot]
    push(first_y.at[low], first_y.at[low], kf_send.at[0], kf_recv.at[0], at_y(1))
    push(first_y.at[high], first_y.at[high], kf_send.at[1], kf_recv.at[1], at_y(-1))
    push(first_y.at[high], first_y.at[high], kf_send.at[2], kf_recv.at[2], at_y(1))
    push(first_y.at[low], first_y.at[low], kf_send.at[3], kf_recv.at[3], at_y(-1))
    own_to_z(0)
    have(19)
    owned = ow.at[tp]
    push(owned, owned, ox_send.at[0], ox_recv.at[0], at_x(1))
    push(owned, owned, ox_send.at[1], ox_recv.at[1], at_x(-1))
    push(owned, owned, ox_send.at[2], ox_recv.at[2], partner)

    take(gath.at[partner_slot], lx_recv.at[2])
    for n, d in ((4, -1), (6, 1), (7, 2)):
        take(gath.at[((x + d) % NX) * NC + (1 - c)], lx_recv.at[n])
    for p in range(NTP // 2):
        pair = jnp.concatenate([gath[2 * p].astype(F32), gath[2 * p + 1].astype(F32)], axis=0)
        xin[2 * ROWS * p : 2 * ROWS * (p + 1), :] = (pair * scale + shift).astype(BF16)

    have(12, 13, 14, 15)
    q_codes = rms(dot(xin[...], qd[...]), qg[...]).astype(BF16)
    q_cont = dot(q_codes, qp[...]) * SCORE
    q_rot = dot(q_codes, qr[...])
    q_rot = (q_rot * tabc[...] + swap_members(q_rot) * tabs[...]) * SCORE
    q_lane = lax.broadcasted_iota(jnp.int32, (SLAB, 128), 1)
    for h in range(4):
        j, rows = h // 2, pl.ds(SLAB * (h % 2), SLAB)
        plain = q_cont[:, 128 * j : 128 * (j + 1)]
        q2[j, rows, 0:128] = jnp.where(q_lane // 64 == h % 2, plain, 0.0).astype(BF16)
        q2[j, rows, 128:256] = jnp.where(q_lane // 32 == h, q_rot, 0.0).astype(BF16)
    below, above = at_slot(0, -1), at_slot(0, 1)
    take(below.at[low], kf_recv.at[0])
    push(below.at[low], below.at[low], ky_send.at[0, 2], ky_recv.at[0, 2], at_y(1))
    take(above.at[high], kf_recv.at[1])
    push(above.at[high], above.at[high], ky_send.at[0, 3], ky_recv.at[0, 3], at_y(-1))

    @pl.when(c == 0)
    def _():
        near_z(1)
        near_z(2)

    take(below.at[high], kf_recv.at[2])
    take(above.at[low], kf_recv.at[3])

    @pl.when(c == 1)
    def _():
        own_to_z(1)
        own_to_z(2)

    have(16)
    sgate[...] = silu(dot(xin[...], gw[...]).astype(BF16).astype(F32))
    from_far(0)
    to_partner(0)

    @pl.when(c == 0)
    def _():
        from_y(1)

    @pl.when(c == 1)
    def _():
        own_to_z(3)

    def halfway(i):
        @pl.when((c == 1) & (i % 2 == 0))
        def _():
            round_z(i + 1)

        @pl.when((c == 1) & (i % 2 == 0) & (i < 6))
        def _():
            round_z(i + 2)

        @pl.when((c == 0) & (i < 7))
        def _():
            from_far(i + 1)

        @pl.when(i < 7)
        def _():
            to_partner(i + 1)

    def one_unit(i, carry):
        @pl.when((c == 0) & (i < 5))
        def _():
            near_z(i + 3)

        @pl.when((c == 0) & (i < 6))
        def _():
            from_y(i + 2)

        @pl.when(i == 1)
        def _():
            gate_to_plane()

        @pl.when(i == OW_MID)
        def _():
            take(ow.at[left], ox_recv.at[0])
            push(ow.at[left, pl.ds(0, 128)], ow.at[left, pl.ds(0, 128)], ox_send.at[3], ox_recv.at[3], at_x(1))
            push(ow.at[left], ow.at[left], ox_send.at[4], ox_recv.at[4], partner)
            take(ow.at[right], ox_recv.at[1])
            push(ow.at[right, pl.ds(128, 128)], ow.at[right, pl.ds(128, 128)], ox_send.at[5], ox_recv.at[5], at_x(-1))
            push(ow.at[right], ow.at[right], ox_send.at[6], ox_recv.at[6], partner)

        @pl.when(i == 7)
        def _():
            take(ow.at[across, pl.ds(0, 128)], ox_recv.at[3])
            take(ow.at[across, pl.ds(128, 128)], ox_recv.at[5])
            push(ow.at[across], ow.at[across], ox_send.at[7], ox_recv.at[7], partner)

        at = z_of(i)
        take(kv.at[at, pl.ds(NY * (1 - c), NY)], kd_recv.at[i])
        codes = jnp.concatenate([kv[at, p, 0:PIECE, :] for p in range(2 * NY)], axis=0)
        rot = jnp.concatenate([kv[at, p, PIECE:MSG, 0:PIECE] for p in range(2 * NY)], axis=1)
        keys = lax.dot_general(ket[...], codes, (((1,), (1,)), ((), ())), preferred_element_type=F32).astype(BF16)
        for j in range(2):
            kt2[j, 0:128, :] = keys[128 * j : 128 * (j + 1)]
            for h in range(4):
                kt2[j, 128 + 32 * h : 160 + 32 * h, :] = rot

        def scores(h):
            return dot(q2[h // 2, SLAB * (h % 2) : SLAB * (h % 2 + 1), :], kt2[h // 2])

        coming = scores(0)
        for h in range(4):
            s = coming
            if h == 2:
                halfway(i)
            if h < 3:
                coming = scores(h + 1)
            rows = pl.ds(SLAB * h, SLAB)
            old = top[rows, :]
            new = jnp.maximum(old, jnp.max(s, axis=1, keepdims=True))
            w = jnp.exp2(s - new)
            fade = jnp.exp2(old - new)
            top[rows, :] = new
            total[rows, :] = total[rows, :] * fade + jnp.sum(w, axis=1, keepdims=True)
            acc[rows, :] = acc[rows, :] * fade + dot(w.astype(BF16), codes)
        return carry

    lax.fori_loop(0, NZ, one_unit, 0)

    have(18)
    col = lax.broadcasted_iota(jnp.int32, (SLAB, COL), 1)
    attended = jnp.zeros((SLAB, COL), F32)
    for h in range(4):
        rows = pl.ds(SLAB * h, SLAB)
        inner = (acc[rows, :] / total[rows, :]).astype(BF16)
        attended = jnp.where(col // 64 == h, dot(inner, ve[...]), attended)
    gated = attended * sgate[...]
    for t in range(NTP):
        gsrc[t] = gated[ROWS * t : ROWS * (t + 1), :].astype(BF16)
    gdst[tp] = gsrc[tp]
    sources = (1, 7, 2, 6, 3, 5, 4)
    for n, d in enumerate(sources):
        push(gsrc.at[(tp + d) % NTP], gdst.at[tp], a_send, a_recv.at[n], at_tp(d))

    have(20, 21)
    from_plane(gbuf, grecv)
    take(zbuf.at[pl.ds(0, NZ - 1)], zsend)
    take(pbuf.at[pl.ds(0, NPLANE - 1)], psend)
    take(gbuf.at[pl.ds(0, NPLANE - 1)], gsend)
    for n in (0, 1, 2, 4, 6, 7):
        take(gath.at[tp], lx_send.at[n])
        take(ow.at[tp], ox_send.at[n])
    for n in (3, 5):
        take(gath.at[tp, :, first], lx_send.at[n])
        take(ow.at[tp, pl.ds(0, 128)], ox_send.at[n])
    here = kv.at[z, slot]

    def sent_along_y(i):
        take(here, ky_send.at[i, 0])
        take(here, ky_send.at[i, 1])
        take(here.at[low], ky_send.at[i, 2])
        take(here.at[high], ky_send.at[i, 3])

    take(here.at[low], kf_send.at[0])
    take(here.at[high], kf_send.at[1])
    take(here.at[high], kf_send.at[2])
    take(here.at[low], kf_send.at[3])
    take(here.at[low], ky_send.at[0, 2])
    take(here.at[high], ky_send.at[0, 3])
    take(kv.at[z, pl.ds(0, NY)], kd_send.at[0])

    def drain(i, carry):
        take(kv.at[z, pl.ds(0, NY)], kd_send.at[i])

        @pl.when(c == 0)
        def _():
            sent_along_y(i)

        @pl.when((c == 1) | (i < 7))
        def _():
            take(here, kz_send.at[i, 0])

        @pl.when(c == 1)
        def _():
            for j in range(1, 4):
                take(here, kz_send.at[i, j])

        return carry

    lax.fori_loop(1, NZ, drain, 0)

    @pl.when(c == 0)
    def _():
        take(here.at[low], kz_send.at[7, 0])
        take(here.at[high], kz_send.at[7, 1])

    take(ow.at[partner_slot], ox_recv.at[2])
    for n, d in ((4, -1), (6, 1), (7, 2)):
        take(ow.at[((x + d) % NX) * NC + (1 - c)], ox_recv.at[n])
    outer = dot(gdst[tp], ow[tp])
    for n, d in enumerate(sources):
        src = (tp - d) % NTP
        take(gdst.at[src], a_recv.at[n])
        outer = outer + dot(gdst[src], ow[src])
    blended = SQRT2 * gath[tp].astype(F32) + vector(0) * outer
    centred = blended - jnp.mean(blended, axis=-1, keepdims=True)
    spread = jnp.mean(centred * centred, axis=-1, keepdims=True)
    out[...] = (centred * lax.rsqrt(spread + EPS) * ng[...] + nb[...]).astype(BF16)
    take(gsrc.at[pl.ds(0, NTP - 1)], a_send)


def per_device(
    latents, context, cond_vec, ctx_vec, shift_w, scale_w, modgate_w, query_down_weight, latent_down_weight, rot_down,
    gate_w, query_norm_gain, latent_norm_gain, query_plain_weight, query_rotary_weight, key_expand_weight,
    value_expand_weight, out_w, norm_gain, norm_bias,
):
    by_slab, by_col = rope_tables()
    args = (
        latents, context, cond_vec.reshape(16, 128), ctx_vec.reshape(16, 128), shift_w, scale_w, modgate_w,
        query_down_weight, latent_down_weight, rot_down.T, gate_w, query_norm_gain.reshape(1, 512),
        latent_norm_gain.reshape(1, COL), query_plain_weight, query_rotary_weight, key_expand_weight,
        value_expand_weight, out_w, norm_gain.reshape(1, WIDTH), norm_bias.reshape(1, WIDTH),
        jnp.asarray(by_slab), jnp.asarray(by_col),
    )
    vm = pltpu.VMEM
    dma = pltpu.SemaphoreType.DMA
    scratch = [
        vm((NTP, ROWS, WIDTH), BF16), vm((32, WIDTH), BF16), vm((16, 128), F32), vm((16, 128), F32),
        vm((3, 64, COL), BF16), vm((WIDTH, 512), BF16), vm((WIDTH, COL), BF16), vm((32, WIDTH), BF16),
        vm((WIDTH, COL), BF16), vm((1, 512), F32), vm((1, COL), F32), vm((512, COL), BF16), vm((512, 128), BF16),
        vm((COL, COL), BF16), vm((COL, COL), BF16), vm((NTP, COL, WIDTH), BF16), vm((1, WIDTH), F32),
        vm((1, WIDTH), F32), vm((16, 128), F32), vm((128, 128), F32),
        vm((NZ, 16, 128), F32), vm((NPLANE, 8, 128), F32), vm((NPLANE, 8, 128), F32), vm((NTP, 8, 128), F32),
        vm((SLAB, WIDTH), BF16),
        vm((SLAB, 128), F32), vm((SLAB, 128), F32), vm((NZ, 2 * NY, MSG, COL), BF16),
        vm((COL, COL), BF16), vm((2, 2 * SLAB, COL), BF16), vm((2, COL, UNIT), BF16), vm((4 * SLAB, COL), F32),
        vm((4 * SLAB, 1), F32), vm((4 * SLAB, 1), F32), vm((SLAB, COL), F32), vm((NTP, ROWS, COL), BF16),
        vm((NTP, ROWS, COL), BF16),
        dma((22,)), dma, dma, dma, dma, dma, dma,
        dma((8,)), dma((8,)), dma((NZ, 4)), dma((NZ, 4)), dma((NZ, 4)), dma((NZ, 4)), dma((NZ,)), dma((NZ,)), dma((4,)), dma((4,)),
        dma((8,)), dma((8,)), dma, dma((NTP - 1,)),
    ]
    return pl.pallas_call(
        body,
        out_shape=pltpu.VMEM((ROWS, WIDTH), BF16),
        in_specs=[pl.BlockSpec(memory_space=pl.ANY)] * len(args),
        out_specs=pl.BlockSpec(memory_space=pltpu.VMEM),
        scratch_shapes=scratch,
        compiler_params=pltpu.CompilerParams(collective_id=0, has_side_effects=True, vmem_limit_bytes=62 * 1024 * 1024),
    )(*args)


def solution(mesh):
    tp, sp = P(None, "tp"), P("sp", "tp")
    return jax.shard_map(
        per_device,
        mesh=mesh,
        in_specs=(
            P(("sp", "tp"), None), P("sp", None), P(), P(), sp, sp, sp, P(), P(), P(), tp, P(), P(), tp, tp, tp, tp,
            P("tp", None), P(), P(),
        ),
        out_specs=P(("sp", "tp"), None),
        check_vma=False,
    )
```

```python
import math

import jax
import jax.numpy as jnp
import numpy as np
from jax import lax
from jax.experimental import pallas as pl
from jax.experimental.pallas import tpu as pltpu
from jax.sharding import PartitionSpec as P

F32, BF16 = jnp.float32, jnp.bfloat16
NZ, NY, NX, NC = 8, 4, 4, 2
NTP = NX * NC
NPLANE = NY * NTP
ROWS = 40
SLAB = 320
HALF = 160
CTXH = 16
PIECE = HALF + CTXH
MSG = PIECE + 32
CUT = 112
UNIT = 2 * NY * PIECE
WIDTH = 2048
COL = 256
EPS = 1e-06
OW_MID = 4
SQRT2 = 2.0**0.5
SCORE = math.log2(math.e) / math.sqrt(96.0)


def rope_tables():
    inverse = (10000.0 ** (-np.arange(8, dtype=np.float64) / 8)).astype(np.float32)
    lane = np.arange(128)
    axis, member, pair = (lane // 16) % 2, (lane // 8) % 2, lane % 8
    sign = np.where(member == 0, -1.0, 1.0)

    def rows_of(numbers, which):
        angle = (numbers[:, None].astype(np.float32) * inverse[pair][None, :]).astype(np.float64)
        keep = axis[None, :] == which
        return np.where(keep, np.cos(angle), 0.0), np.where(keep, np.sin(angle) * sign, 0.0)

    cos_row, sin_row = rows_of(np.arange(160), 0)
    cos_col, sin_col = rows_of(np.arange(64), 1)
    by_slab = np.zeros((32, 16, 128), np.float32)
    by_slab[:, 0:5] = cos_row.reshape(32, 5, 128)
    by_slab[:, 8:13] = sin_row.reshape(32, 5, 128)
    return by_slab, np.concatenate([cos_col, sin_col], 0).astype(np.float32)


def dot(a, b):
    return jnp.dot(a, b, preferred_element_type=F32)


def silu(v):
    return v / (1.0 + jnp.exp(-v))


def rms(v, gain):
    return v * lax.rsqrt(jnp.mean(v * v, axis=-1, keepdims=True) + EPS) * gain


def swap_members(v):
    lane = lax.broadcasted_iota(jnp.int32, v.shape, 1)
    return jnp.where(lane % 16 < 8, pltpu.roll(v, 120, 1), pltpu.roll(v, 8, 1))


def body(
    lat_h, ctx_h, cond_h, ctxv_h, shw_h, scw_h, mgw_h, qd_h, ld_h, rd_h, gw_h, qg_h, kg_h, qp_h, qr_h, ke_h, ve_h,
    ow_h, ng_h, nb_h, rrow_h, rcol_h, out,
    gath, ctx_v, cond_v, ctxv_v, w3, qd, ld, rd, gw, qg, kg, qp, qr, ke, ve, ow, ng, nb, rrow, rcol,
    zbuf, pbuf, gbuf, mod, xin, tabc, tabs, kv, ket, q2, kt2, acc, top, total, sgate, gsrc, gdst,
    lsem, zsend, zrecv, psend, precv, gsend, grecv, lx_send, lx_recv, kz_send, kz_recv, ky_send, ky_recv,
    kd_send, kd_recv, kf_send, kf_recv, ox_send, ox_recv, a_send, a_recv,
):
    sp, tp = lax.axis_index("sp"), lax.axis_index("tp")
    z, y, x, c = sp // NY, sp % NY, tp // NC, tp % NC

    def at_z(d):
        return {"sp": ((z + d) % NZ) * NY + y, "tp": tp}

    def at_y(d):
        return {"sp": z * NY + (y + d) % NY, "tp": tp}

    def slot_x(d):
        return ((x + d) % NX) * NC + c

    def at_x(d):
        return {"sp": sp, "tp": slot_x(d)}

    partner_slot = x * NC + (1 - c)
    partner = {"sp": sp, "tp": partner_slot}

    def at_tp(d):
        return {"sp": sp, "tp": (tp + d) % NTP}

    def push(src, dst, send, recv, to):
        pltpu.make_async_remote_copy(
            src_ref=src, dst_ref=dst, send_sem=send, recv_sem=recv, device_id=to, device_id_type=pl.DeviceIdType.MESH
        ).start()

    def take(ref, sem):
        pltpu.make_async_copy(ref, ref, sem).wait()

    local = [
        (cond_h, cond_v), (ctxv_h, ctxv_v), (shw_h, w3.at[0]), (scw_h, w3.at[1]), (mgw_h, w3.at[2]),
        (lat_h, gath.at[tp]), (ctx_h, ctx_v), (ld_h, ld), (rd_h, rd), (rrow_h.at[sp], rrow), (rcol_h, rcol),
        (kg_h, kg), (qd_h, qd), (qg_h, qg), (qp_h, qp), (qr_h, qr), (gw_h, gw), (ke_h, ke), (ve_h, ve),
        (ow_h, ow.at[tp]), (ng_h, ng), (nb_h, nb),
    ]
    for k, (src, dst) in enumerate(local):
        pltpu.make_async_copy(src, dst, lsem.at[k]).start()

    def have(*which):
        for k in which:
            take(local[k][1], lsem.at[k])

    barrier = pltpu.get_barrier_semaphore()
    plane = [(dy, dt) for dy in range(NY) for dt in range(NTP) if (dy, dt) != (0, 0)]
    plane.sort(key=lambda at: -min(at[0], NY - at[0]) - min(at[1], NTP - at[1]) / 2)

    def at_plane(dy, dt):
        return {"sp": z * NY + (y + dy) % NY, "tp": (tp + dt) % NTP}

    peers = [at_z(d) for d in range(1, NZ)] + [at_plane(dy, dt) for dy, dt in plane]
    for peer in peers:
        pl.semaphore_signal(barrier, inc=1, device_id=peer, device_id_type=pl.DeviceIdType.MESH)

    have(0, 1, 2, 3, 4)
    pick = pl.ds(sp // 2, 1)
    lane = lax.broadcasted_iota(jnp.int32, (8, 128), 1)
    line = lax.broadcasted_iota(jnp.int32, (8, 128), 0)
    mine = lane // 64 == sp % 2
    cond_row = jnp.broadcast_to(silu(cond_v[pick, :]), (8, 128))
    ctxv_row = jnp.broadcast_to(silu(ctxv_v[pick, :]), (8, 128))
    part = jnp.zeros((8, COL), F32)
    for k in range(3):
        at = 2 * k
        rows = jnp.where(line == at, cond_row, jnp.where(line == at + 1, ctxv_row, 0.0))
        rows = jnp.where(mine, rows, 0.0).astype(BF16)
        part = part + dot(rows, jnp.concatenate([w3[k], w3[k]], axis=0))
    zbuf[z] = jnp.concatenate([part[0:4, 0:128], part[0:4, 128:256], part[4:8, 0:128], part[4:8, 128:256]], axis=0)
    pl.semaphore_wait(barrier, len(peers))

    for d in (4, 3, 5, 2, 6, 1, 7):
        push(zbuf.at[z], zbuf.at[z], zsend, zrecv, at_z(d))
    have(5)
    own = gath.at[tp]
    push(own, own, lx_send.at[0], lx_recv.at[0], at_x(1))
    push(own, own, lx_send.at[1], lx_recv.at[1], at_x(-1))
    push(own, own, lx_send.at[2], lx_recv.at[2], partner)
    left, right, across = slot_x(-1), slot_x(1), slot_x(2)
    first, second = pl.ds(0, WIDTH // 2), pl.ds(WIDTH // 2, WIDTH // 2)
    take(gath.at[left], lx_recv.at[0])
    push(gath.at[left, :, first], gath.at[left, :, first], lx_send.at[3], lx_recv.at[3], at_x(1))
    push(gath.at[left], gath.at[left], lx_send.at[4], lx_recv.at[4], partner)
    take(gath.at[right], lx_recv.at[1])
    push(gath.at[right, :, second], gath.at[right, :, second], lx_send.at[5], lx_recv.at[5], at_x(-1))
    push(gath.at[right], gath.at[right], lx_send.at[6], lx_recv.at[6], partner)

    take(zbuf.at[pl.ds(0, NZ - 1)], zrecv)
    whole = zbuf[0]
    for k in range(1, NZ):
        whole = whole + zbuf[k]
    me = y * NTP + tp
    pbuf[me] = whole[0:8]
    gbuf[me] = whole[8:16]
    for dy, dt in plane:
        push(pbuf.at[me], pbuf.at[me], psend, precv, at_plane(dy, dt))

    def gate_to_plane():
        for dy, dt in plane:
            push(gbuf.at[me], gbuf.at[me], gsend, grecv, at_plane(dy, dt))

    have(9, 10, 17)
    for k in range(5):
        rows = pl.ds(64 * k, 64)
        tabc[rows, :] = rrow[k : k + 1, :] + rcol[0:64, :]
        tabs[rows, :] = rrow[8 + k : 9 + k, :] + rcol[64:128, :]
    ket[...] = ke[...].astype(F32).T.astype(BF16)
    top[...] = jnp.full(top.shape, -1e30, F32)
    total[...] = jnp.zeros(total.shape, F32)
    acc[...] = jnp.zeros(acc.shape, F32)

    take(gath.at[across, :, first], lx_recv.at[3])
    take(gath.at[across, :, second], lx_recv.at[5])
    push(gath.at[across], gath.at[across], lx_send.at[7], lx_recv.at[7], partner)

    def from_plane(buf, sem):
        take(buf.at[pl.ds(0, NPLANE - 1)], sem)
        for t in range(NTP):
            mod[t] = (buf[t] + buf[NTP + t]) + (buf[2 * NTP + t] + buf[3 * NTP + t])

    from_plane(pbuf, precv)
    def vector(row):
        return jnp.concatenate([mod[t, r : r + 1, :] for t in range(NTP) for r in (row, row + 4)], axis=1)

    shift, scale = vector(0), 1.0 + vector(2)
    have(6, 7, 8, 11)
    lines = [gath[NC * k + c].astype(F32) for k in range(NX)]
    mine_lat = jnp.concatenate(lines, axis=0) * scale + shift
    mine_ctx = ctx_v[pl.ds(pl.multiple_of(CTXH * c, CTXH), CTXH), :].astype(F32) * (1.0 + vector(3)) + vector(1)
    mine_in = jnp.concatenate([mine_lat, mine_ctx], axis=0).astype(BF16)
    slot = NY * c + y
    kv[z, slot, 0:PIECE, :] = rms(dot(mine_in, ld[...]), kg[...]).astype(BF16)
    flat = lax.dot_general(mine_in, rd[...], (((1,), (1,)), ((), ())), preferred_element_type=F32)
    flat = jnp.concatenate([flat, jnp.zeros((PIECE, 96), F32)], axis=1)
    lat_part = flat[0:HALF]

    def rows_of(table):
        return jnp.concatenate(
            [table[pl.ds(pl.multiple_of(ROWS * (NC * k + c), 8), ROWS), :] for k in range(NX)], axis=0
        )

    turned = lat_part * rows_of(tabc) + swap_members(lat_part) * rows_of(tabs)
    both = jnp.concatenate([turned, flat[HALF:], jnp.zeros((256 - PIECE, 128), F32)], axis=0)
    kv[z, slot, PIECE:MSG, :] = both.T[0:32, :].astype(BF16)

    def z_of(i):
        off = (i % 2) * ((i + 1) // 2) - (1 - i % 2) * (i // 2)
        return (z + off + NZ) % NZ

    low, high = pl.ds(0, CUT), pl.ds(CUT, MSG - CUT)

    def z_back(i):
        return {"sp": ((z + NZ + 1 - 2 * (i % 2)) % NZ) * NY + y, "tp": tp}

    def at_slot(i, d):
        return kv.at[z_of(i), NY * c + (y + d + NY) % NY]

    def near_z(i):
        here = at_slot(i, 0)

        @pl.when(i < 7)
        def _():
            take(here, kz_recv.at[i, 0])

        @pl.when(i == 7)
        def _():
            take(here.at[low], kz_recv.at[7, 0])
            take(here.at[high], kz_recv.at[7, 1])

        @pl.when(i < 5)
        def _():
            push(here, here, kz_send.at[i + 2, 0], kz_recv.at[i + 2, 0], z_back(i))

        @pl.when(i == 5)
        def _():
            push(here.at[low], here.at[low], kz_send.at[7, 0], kz_recv.at[7, 0], at_z(-1))

        @pl.when(i == 6)
        def _():
            push(here.at[high], here.at[high], kz_send.at[7, 1], kz_recv.at[7, 1], at_z(1))

        to_y(i)

    def to_y(i):
        here = at_slot(i, 0)
        push(here, here, ky_send.at[i, 0], ky_recv.at[i, 0], at_y(1))
        push(here, here, ky_send.at[i, 1], ky_recv.at[i, 1], at_y(-1))

    def from_y(i):
        below, above = at_slot(i, -1), at_slot(i, 1)
        take(below, ky_recv.at[i, 0])
        push(below.at[low], below.at[low], ky_send.at[i, 2], ky_recv.at[i, 2], at_y(1))
        take(above, ky_recv.at[i, 1])
        push(above.at[high], above.at[high], ky_send.at[i, 3], ky_recv.at[i, 3], at_y(-1))

    def from_far(i):
        far = at_slot(i, 2)
        take(far.at[low], ky_recv.at[i, 2])
        take(far.at[high], ky_recv.at[i, 3])

    def to_partner(i):
        four = kv.at[z_of(i), pl.ds(NY * c, NY)]
        push(four, four, kd_send.at[i], kd_recv.at[i], partner)

    turn = (0, 1, -1, 2)

    def own_to_z(j):
        here = at_slot(0, turn[j])
        push(here, here, kz_send.at[1, j], kz_recv.at[1, j], at_z(-1))
        push(here, here, kz_send.at[2, j], kz_recv.at[2, j], at_z(1))

    def round_z(i):
        for j in range(4):
            here = at_slot(i, turn[j])
            take(here, kz_recv.at[i, j])

            @pl.when((i < 5) | ((i == 5) & (j < 2)) | ((i == 6) & (j >= 2)))
            def _(here=here, j=j):
                n = jnp.minimum(i + 2, 7)
                push(here, here, kz_send.at[n, j], kz_recv.at[n, j], z_back(i))

    first_y = kv.at[z, slot]
    push(first_y.at[low], first_y.at[low], kf_send.at[0], kf_recv.at[0], at_y(1))
    push(first_y.at[high], first_y.at[high], kf_send.at[1], kf_recv.at[1], at_y(-1))
    push(first_y.at[high], first_y.at[high], kf_send.at[2], kf_recv.at[2], at_y(1))
    push(first_y.at[low], first_y.at[low], kf_send.at[3], kf_recv.at[3], at_y(-1))
    own_to_z(0)
    have(19)
    owned = ow.at[tp]
    push(owned, owned, ox_send.at[0], ox_recv.at[0], at_x(1))
    push(owned, owned, ox_send.at[1], ox_recv.at[1], at_x(-1))
    push(owned, owned, ox_send.at[2], ox_recv.at[2], partner)

    take(gath.at[partner_slot], lx_recv.at[2])
    for n, d in ((4, -1), (6, 1), (7, 2)):
        take(gath.at[((x + d) % NX) * NC + (1 - c)], lx_recv.at[n])
    for p in range(NTP // 2):
        pair = jnp.concatenate([gath[2 * p].astype(F32), gath[2 * p + 1].astype(F32)], axis=0)
        xin[2 * ROWS * p : 2 * ROWS * (p + 1), :] = (pair * scale + shift).astype(BF16)

    have(12, 13, 14, 15)
    q_codes = rms(dot(xin[...], qd[...]), qg[...]).astype(BF16)
    q_cont = dot(q_codes, qp[...]) * SCORE
    q_rot = dot(q_codes, qr[...])
    q_rot = (q_rot * tabc[...] + swap_members(q_rot) * tabs[...]) * SCORE
    q_lane = lax.broadcasted_iota(jnp.int32, (SLAB, 128), 1)
    for h in range(4):
        j, rows = h // 2, pl.ds(SLAB * (h % 2), SLAB)
        plain = q_cont[:, 128 * j : 128 * (j + 1)]
        q2[j, rows, 0:128] = jnp.where(q_lane // 64 == h % 2, plain, 0.0).astype(BF16)
        q2[j, rows, 128:256] = jnp.where(q_lane // 32 == h, q_rot, 0.0).astype(BF16)
    below, above = at_slot(0, -1), at_slot(0, 1)
    take(below.at[low], kf_recv.at[0])
    push(below.at[low], below.at[low], ky_send.at[0, 2], ky_recv.at[0, 2], at_y(1))
    take(above.at[high], kf_recv.at[1])
    push(above.at[high], above.at[high], ky_send.at[0, 3], ky_recv.at[0, 3], at_y(-1))

    @pl.when(c == 0)
    def _():
        near_z(1)
        near_z(2)

    take(below.at[high], kf_recv.at[2])
    take(above.at[low], kf_recv.at[3])

    @pl.when(c == 1)
    def _():
        own_to_z(1)
        own_to_z(2)

    have(16)
    sgate[...] = silu(dot(xin[...], gw[...]).astype(BF16).astype(F32))
    from_far(0)
    to_partner(0)

    @pl.when(c == 0)
    def _():
        from_y(1)

    @pl.when(c == 1)
    def _():
        own_to_z(3)

    def halfway(i):
        @pl.when((c == 1) & (i % 2 == 0))
        def _():
            round_z(i + 1)

        @pl.when((c == 1) & (i % 2 == 0) & (i < 6))
        def _():
            round_z(i + 2)

        @pl.when((c == 0) & (i < 7))
        def _():
            from_far(i + 1)

        @pl.when(i < 7)
        def _():
            to_partner(i + 1)

    def one_unit(i, carry):
        @pl.when((c == 0) & (i < 5))
        def _():
            near_z(i + 3)

        @pl.when((c == 0) & (i < 6))
        def _():
            from_y(i + 2)

        @pl.when(i == 1)
        def _():
            gate_to_plane()

        @pl.when(i == OW_MID)
        def _():
            take(ow.at[left], ox_recv.at[0])
            push(ow.at[left, pl.ds(0, 128)], ow.at[left, pl.ds(0, 128)], ox_send.at[3], ox_recv.at[3], at_x(1))
            push(ow.at[left], ow.at[left], ox_send.at[4], ox_recv.at[4], partner)
            take(ow.at[right], ox_recv.at[1])
            push(ow.at[right, pl.ds(128, 128)], ow.at[right, pl.ds(128, 128)], ox_send.at[5], ox_recv.at[5], at_x(-1))
            push(ow.at[right], ow.at[right], ox_send.at[6], ox_recv.at[6], partner)

        @pl.when(i == 7)
        def _():
            take(ow.at[across, pl.ds(0, 128)], ox_recv.at[3])
            take(ow.at[across, pl.ds(128, 128)], ox_recv.at[5])
            push(ow.at[across], ow.at[across], ox_send.at[7], ox_recv.at[7], partner)

        at = z_of(i)
        take(kv.at[at, pl.ds(NY * (1 - c), NY)], kd_recv.at[i])
        codes = jnp.concatenate([kv[at, p, 0:PIECE, :] for p in range(2 * NY)], axis=0)
        rot = jnp.concatenate([kv[at, p, PIECE:MSG, 0:PIECE] for p in range(2 * NY)], axis=1)
        keys = lax.dot_general(ket[...], codes, (((1,), (1,)), ((), ())), preferred_element_type=F32).astype(BF16)
        for j in range(2):
            kt2[j, 0:128, :] = keys[128 * j : 128 * (j + 1)]
            for h in range(4):
                kt2[j, 128 + 32 * h : 160 + 32 * h, :] = rot

        def scores(h):
            return dot(q2[h // 2, SLAB * (h % 2) : SLAB * (h % 2 + 1), :], kt2[h // 2])

        coming = scores(0)
        for h in range(4):
            s = coming
            if h == 2:
                halfway(i)
            if h < 3:
                coming = scores(h + 1)
            rows = pl.ds(SLAB * h, SLAB)
            old = top[rows, :]
            new = jnp.maximum(old, jnp.max(s, axis=1, keepdims=True))
            w = jnp.exp2(s - new)
            fade = jnp.exp2(old - new)
            top[rows, :] = new
            total[rows, :] = total[rows, :] * fade + jnp.sum(w, axis=1, keepdims=True)
            acc[rows, :] = acc[rows, :] * fade + dot(w.astype(BF16), codes)
        return carry

    lax.fori_loop(0, NZ, one_unit, 0)

    have(18)
    col = lax.broadcasted_iota(jnp.int32, (SLAB, COL), 1)
    attended = jnp.zeros((SLAB, COL), F32)
    for h in range(4):
        rows = pl.ds(SLAB * h, SLAB)
        inner = (acc[rows, :] / total[rows, :]).astype(BF16)
        attended = jnp.where(col // 64 == h, dot(inner, ve[...]), attended)
    gated = attended * sgate[...]
    for t in range(NTP):
        gsrc[t] = gated[ROWS * t : ROWS * (t + 1), :].astype(BF16)
    gdst[tp] = gsrc[tp]
    sources = (1, 7, 2, 6, 3, 5, 4)
    for n, d in enumerate(sources):
        push(gsrc.at[(tp + d) % NTP], gdst.at[tp], a_send, a_recv.at[n], at_tp(d))

    have(20, 21)
    from_plane(gbuf, grecv)
    take(zbuf.at[pl.ds(0, NZ - 1)], zsend)
    take(pbuf.at[pl.ds(0, NPLANE - 1)], psend)
    take(gbuf.at[pl.ds(0, NPLANE - 1)], gsend)
    for n in (0, 1, 2, 4, 6, 7):
        take(gath.at[tp], lx_send.at[n])
        take(ow.at[tp], ox_send.at[n])
    for n in (3, 5):
        take(gath.at[tp, :, first], lx_send.at[n])
        take(ow.at[tp, pl.ds(0, 128)], ox_send.at[n])
    here = kv.at[z, slot]

    def sent_along_y(i):
        take(here, ky_send.at[i, 0])
        take(here, ky_send.at[i, 1])
        take(here.at[low], ky_send.at[i, 2])
        take(here.at[high], ky_send.at[i, 3])

    take(here.at[low], kf_send.at[0])
    take(here.at[high], kf_send.at[1])
    take(here.at[high], kf_send.at[2])
    take(here.at[low], kf_send.at[3])
    take(here.at[low], ky_send.at[0, 2])
    take(here.at[high], ky_send.at[0, 3])
    take(kv.at[z, pl.ds(0, NY)], kd_send.at[0])

    def drain(i, carry):
        take(kv.at[z, pl.ds(0, NY)], kd_send.at[i])

        @pl.when(c == 0)
        def _():
            sent_along_y(i)

        @pl.when((c == 1) | (i < 7))
        def _():
            take(here, kz_send.at[i, 0])

        @pl.when(c == 1)
        def _():
            for j in range(1, 4):
                take(here, kz_send.at[i, j])

        return carry

    lax.fori_loop(1, NZ, drain, 0)

    @pl.when(c == 0)
    def _():
        take(here.at[low], kz_send.at[7, 0])
        take(here.at[high], kz_send.at[7, 1])

    take(ow.at[partner_slot], ox_recv.at[2])
    for n, d in ((4, -1), (6, 1), (7, 2)):
        take(ow.at[((x + d) % NX) * NC + (1 - c)], ox_recv.at[n])
    outer = dot(gdst[tp], ow[tp])
    for n, d in enumerate(sources):
        src = (tp - d) % NTP
        take(gdst.at[src], a_recv.at[n])
        outer = outer + dot(gdst[src], ow[src])
    blended = SQRT2 * gath[tp].astype(F32) + vector(0) * outer
    centred = blended - jnp.mean(blended, axis=-1, keepdims=True)
    spread = jnp.mean(centred * centred, axis=-1, keepdims=True)
    out[...] = (centred * lax.rsqrt(spread + EPS) * ng[...] + nb[...]).astype(BF16)
    take(gsrc.at[pl.ds(0, NTP - 1)], a_send)


def per_device(
    latents, context, cond_vec, ctx_vec, shift_w, scale_w, modgate_w, query_down_weight, latent_down_weight, rot_down,
    gate_w, query_norm_gain, latent_norm_gain, query_plain_weight, query_rotary_weight, key_expand_weight,
    value_expand_weight, out_w, norm_gain, norm_bias,
):
    by_slab, by_col = rope_tables()
    args = (
        latents, context, cond_vec.reshape(16, 128), ctx_vec.reshape(16, 128), shift_w, scale_w, modgate_w,
        query_down_weight, latent_down_weight, rot_down.T, gate_w, query_norm_gain.reshape(1, 512),
        latent_norm_gain.reshape(1, COL), query_plain_weight, query_rotary_weight, key_expand_weight,
        value_expand_weight, out_w, norm_gain.reshape(1, WIDTH), norm_bias.reshape(1, WIDTH),
        jnp.asarray(by_slab), jnp.asarray(by_col),
    )
    vm = pltpu.VMEM
    dma = pltpu.SemaphoreType.DMA
    scratch = [
        vm((NTP, ROWS, WIDTH), BF16), vm((32, WIDTH), BF16), vm((16, 128), F32), vm((16, 128), F32),
        vm((3, 64, COL), BF16), vm((WIDTH, 512), BF16), vm((WIDTH, COL), BF16), vm((32, WIDTH), BF16),
        vm((WIDTH, COL), BF16), vm((1, 512), F32), vm((1, COL), F32), vm((512, COL), BF16), vm((512, 128), BF16),
        vm((COL, COL), BF16), vm((COL, COL), BF16), vm((NTP, COL, WIDTH), BF16), vm((1, WIDTH), F32),
        vm((1, WIDTH), F32), vm((16, 128), F32), vm((128, 128), F32),
        vm((NZ, 16, 128), F32), vm((NPLANE, 8, 128), F32), vm((NPLANE, 8, 128), F32), vm((NTP, 8, 128), F32),
        vm((SLAB, WIDTH), BF16),
        vm((SLAB, 128), F32), vm((SLAB, 128), F32), vm((NZ, 2 * NY, MSG, COL), BF16),
        vm((COL, COL), BF16), vm((2, 2 * SLAB, COL), BF16), vm((2, COL, UNIT), BF16), vm((4 * SLAB, COL), F32),
        vm((4 * SLAB, 1), F32), vm((4 * SLAB, 1), F32), vm((SLAB, COL), F32), vm((NTP, ROWS, COL), BF16),
        vm((NTP, ROWS, COL), BF16),
        dma((22,)), dma, dma, dma, dma, dma, dma,
        dma((8,)), dma((8,)), dma((NZ, 4)), dma((NZ, 4)), dma((NZ, 4)), dma((NZ, 4)), dma((NZ,)), dma((NZ,)), dma((4,)), dma((4,)),
        dma((8,)), dma((8,)), dma, dma((NTP - 1,)),
    ]
    return pl.pallas_call(
        body,
        out_shape=pltpu.VMEM((ROWS, WIDTH), BF16),
        in_specs=[pl.BlockSpec(memory_space=pl.ANY)] * len(args),
        out_specs=pl.BlockSpec(memory_space=pltpu.VMEM),
        scratch_shapes=scratch,
        compiler_params=pltpu.CompilerParams(collective_id=0, has_side_effects=True, vmem_limit_bytes=62 * 1024 * 1024),
    )(*args)


def solution(mesh):
    tp, sp = P(None, "tp"), P("sp", "tp")
    return jax.shard_map(
        per_device,
        mesh=mesh,
        in_specs=(
            P(("sp", "tp"), None), P("sp", None), P(), P(), sp, sp, sp, P(), P(), P(), tp, P(), P(), tp, tp, tp, tp,
            P("tp", None), P(), P(),
        ),
        out_specs=P(("sp", "tp"), None),
        check_vma=False,
    )
```
